256 devices in a mesh: sp: 64 (over z, x, core), tp: 4 (over y).
Axes of the slice: x: 4, y: 4, z: 8, core: 2. Of those that a mesh axis runs over, the one named last changes fastest.
Arguments:
- query_rows: bfloat16 [16384, 2048], P('sp', 'tp'), may hold values from -6 to 6
- key_rows: bfloat16 [16384, 2048], P('sp', 'tp'), may hold values from -6 to 6
- value_rows: bfloat16 [16384, 2048], P('sp', 'tp'), may hold values from -6 to 6
- gate_rows: bfloat16 [16384, 2048], P('sp', 'tp'), may hold values from -6 to 6
- log_decay: float32 [16384, 16], P('sp', 'tp'), may hold values from -1 to 0
- head_gain: float32 [2048], P('tp'), may hold values from 0.1 to 1.9
- out_weight: bfloat16 [2048, 2048], P('tp'), may hold values from -0.125 to 0.125
- residual: bfloat16 [16384, 2048], P(('sp', 'tp')), may hold values from -6 to 6
- ffn_gain: float32 [2048], replicated, may hold values from 0.1 to 1.9
- gate_weight: bfloat16 [64, 2048, 2048], P('sp', None, 'tp'), may hold values from -0.375 to 0.375
- up_weight: bfloat16 [64, 2048, 2048], P('sp', None, 'tp'), may hold values from -0.375 to 0.375
- down_weight: bfloat16 [64, 2048, 2048], P('sp', 'tp'), may hold values from -0.01953125 to 0.01953125
- routes: int32 [16384, 4], P('sp'), may hold values from 0 to 63, all different within a row; in each aligned block of 64 rows (0 to 63, 64 to 127, ...) at most 6 rows name the same one
- route_weights: float32 [16384, 4], P(('sp', 'tp')), may hold values from 0.05 to 1
Outputs:
- layer_out: bfloat16 [16384, 2048], P(('sp', 'tp'))
The draws below stay inside these ranges and needn't reach their ends.
Inputs may be any that keep to these rules, and one draw needn't show every extreme that they name: `routes`: each row names 4 different experts. In each aligned block of 64 rows no expert is named by more than 6 rows, and in some block some expert is named by exactly 6 rows.
All inputs are finite; a program needn't handle non-finite values.
Results may differ from the reference program's by a relative error of at most 0.014.
Values may be sent and summed in bfloat16 or wider, within the bound.
No kernel may reach another device: no remote copies, remote signals or barrier semaphores. Data moves between devices by JAX's collectives and lax.ppermute only.
A program may use at most 128 MiB of HBM per device.

```python
import math
from functools import partial
import jax
import jax.numpy as jnp
import numpy as np
from jax import lax

D = 2048
HEAD_TOTAL = 16
HEAD_DIM = 128
FF = 2048
TOPK = 4
BLOCK = 128
TOK_DEV = 256
RET_WIDTH = 2048
EXPERTS = 64
TOKEN_TOTAL = 16384
ROWS_DEV = 64
CAP = 6
N_TP = 4


def draw_log_decay(key, part):
    split_random_keys = jax.random.split(jax.random.fold_in(key, 17), 7)
    fast_share = 0.5
    is_fast = jax.random.uniform(split_random_keys[0], (HEAD_TOTAL,), jnp.float32) < fast_share
    fast_rate = jnp.exp(jax.random.uniform(split_random_keys[1], (HEAD_TOTAL,), jnp.float32, math.log(1.0 / 15.0), math.log(1.0 / 8.0)))
    slow_rate = jnp.exp(jax.random.uniform(split_random_keys[2], (HEAD_TOTAL,), jnp.float32, math.log(0.05), math.log(0.25))) / TOKEN_TOTAL
    baseline_rate = jnp.where(is_fast, fast_rate, slow_rate)
    span_count = TOKEN_TOTAL // TOK_DEV
    extent_factor = jnp.exp(jax.random.uniform(split_random_keys[3], (span_count, HEAD_TOTAL), jnp.float32, -math.log(2.0), math.log(2.0)))
    extent_factor = jnp.repeat(extent_factor, TOK_DEV, axis=0)
    coarse_factor = jax.random.uniform(split_random_keys[4], (TOKEN_TOTAL, HEAD_TOTAL), jnp.float32, 0.5, 1.5)
    spike_position = jax.random.randint(split_random_keys[5], (3,), 0, TOKEN_TOTAL)
    spike_flags = jnp.zeros((TOKEN_TOTAL,), jnp.float32).at[spike_position].set(1.0)
    spike_penalty = jnp.log(jax.random.uniform(split_random_keys[6], (HEAD_TOTAL,), jnp.float32, 0.6, 0.8))
    return (-baseline_rate[None, :] * extent_factor * coarse_factor + spike_flags[:, None] * spike_penalty[None, :]).astype(jnp.float32)


def steps_of(rng, extent, shards, low, high):
    def one(dim, shards_of):
        heights = jax.random.uniform(jax.random.fold_in(jax.random.fold_in(rng, 6), dim), (shards_of,), jnp.float32, low / len(shards), high / len(shards))
        return jnp.repeat(jnp.exp(heights), extent[dim] // shards_of).reshape((-1,) + (1,) * (len(extent) - dim - 1))

    gain = one(*shards[0])
    for cut in shards[1:]:
        gain = gain * one(*cut)
    return gain


def deal_out(key, own, number, rows, amount, top, limit, lean):
    sequence = jax.random.permutation(key, amount)
    crowded, common = shares(amount, rows * top, limit, lean, True), shares(amount, rows * top, limit, lean, False)
    places = jnp.arange(amount)

    def named(lengths, rotation):
        used = int((lengths > 0).sum())
        fixed = max(1, used // 4)
        moved = fixed + (places - fixed + rotation * (used - fixed)) % max(1, amount - fixed)
        return jnp.zeros((amount,), jnp.int32).at[sequence[jnp.where(places < fixed, places, moved)]].set(jnp.asarray(lengths, jnp.int32))

    lengths = jnp.where(number % 4 == 0, named(crowded, number // 4), named(common, number - number // 4 - 1))
    mixed = jax.random.permutation(jax.random.fold_in(own, 3), amount)
    giver, receiver = mixed[0:amount // 2 * 2:2], mixed[1:amount // 2 * 2:2]
    margin = jnp.minimum(lengths[giver] - 1, limit - lengths[receiver]) // 2
    margin = jnp.where((giver == sequence[0]) | (receiver == sequence[0]) | (lengths[receiver] == 0), 0, jnp.maximum(margin, 0))
    moved = jax.random.randint(jax.random.fold_in(own, 4), (amount // 2,), 0, 1 << 20) % (margin + 1)
    lengths = lengths.at[giver].add(-moved).at[receiver].add(moved)
    members = jnp.searchsorted(jnp.cumsum(lengths), jnp.arange(rows * top), side="right").astype(jnp.int32)
    grid = members.reshape(top, rows).T
    grid = grid[jax.random.permutation(jax.random.fold_in(own, 1), rows)]
    rotation = jax.random.randint(jax.random.fold_in(own, 2), (rows, 1), 0, top)
    return jnp.take_along_axis(grid, (jnp.arange(top)[None, :] + rotation) % top, axis=1)


def shares(number_of, total, limit, skew, full):
    weights = [(1 << 20) // math.isqrt(rank ** skew) + 1 for rank in range(1, number_of + 1)]
    largest = limit if full else min(limit, max(-(-total // number_of), total * weights[0] // sum(weights)))
    least = 1 if total - largest >= number_of - 1 else 0
    holding, rest = [largest] + [least] * (number_of - 1), total - largest - least * (number_of - 1)
    while rest > 0:
        candidates = [i for i in range(1, number_of) if holding[i] < largest] or [i for i in range(1, number_of) if holding[i] < limit]
        whole, left = sum([weights[i] for i in candidates]), rest
        for i in candidates:
            addition = min(limit - holding[i], max(1, left * weights[i] // whole), rest)
            holding[i] = holding[i] + addition
            rest = rest - addition
    return np.array(holding)


def scatter_about(own_key, shape, scale, most, cuts=(), kind=jnp.bfloat16):
    entries = jax.random.normal(own_key, shape, jnp.float32) * scale
    if len(cuts) > 0:
        entries = steps_of(own_key, shape, cuts, -0.22, 0.18) * entries
    return jnp.clip(entries, min=-most, max=most).astype(kind)


def setup_inputs(seed: int = 0) -> dict:
    key_list = jax.random.split(jax.random.key(seed), 15)
    query_rows = scatter_about(key_list[0], (TOKEN_TOTAL, RET_WIDTH), 1.0, 6.0, ((0, 64), (1, 4)))
    key_rows = scatter_about(key_list[1], (TOKEN_TOTAL, RET_WIDTH), 1.0, 6.0, ((0, 64), (1, 4)))
    value_rows = scatter_about(key_list[2], (TOKEN_TOTAL, RET_WIDTH), 1.0, 6.0, ((0, 64), (1, 4)))
    gate_rows = scatter_about(key_list[3], (TOKEN_TOTAL, RET_WIDTH), 1.0, 6.0, ((0, 64), (1, 4)))
    log_decay = draw_log_decay(jax.random.fold_in(key_list[14], 71), 0)
    head_gain = jnp.clip(1.0 + 0.18 * jax.random.normal(key_list[5], (RET_WIDTH,), jnp.float32), 0.1, 1.9)
    out_weight = scatter_about(key_list[6], (RET_WIDTH, D), RET_WIDTH ** -0.5, 0.125, ((0, 4),))
    residual = scatter_about(key_list[7], (TOKEN_TOTAL, D), 1.0, 6.0, ((0, 256),))
    ffn_gain = jnp.clip(1.0 + 0.18 * jax.random.normal(key_list[8], (D,), jnp.float32), 0.1, 1.9)
    gate_weight = scatter_about(key_list[9], (EXPERTS, D, FF), (D // 9) ** -0.5, 0.375, ((0, 64), (2, 4)))
    up_weight = scatter_about(key_list[10], (EXPERTS, D, FF), (D // 9) ** -0.5, 0.375, ((0, 64), (2, 4)))
    down_weight = scatter_about(key_list[11], (EXPERTS, FF, D), (FF * 44) ** -0.5, 0.01953125, ((0, 64), (1, 4)))
    routes_keys = jax.random.split(jax.random.fold_in(key_list[12], 1), TOKEN_TOTAL // ROWS_DEV)
    routes_turns = jax.random.permutation(jax.random.fold_in(key_list[12], 3), TOKEN_TOTAL // ROWS_DEV)
    routes = jax.vmap(lambda own, number: deal_out(jax.random.fold_in(key_list[12], 2), own, number, ROWS_DEV, EXPERTS, TOPK, CAP, 1))(routes_keys, routes_turns).reshape((TOKEN_TOTAL, TOPK))
    route_weights = jnp.clip(jnp.exp(math.log(1.0) - 2.9957323 * jax.random.uniform(key_list[13], (TOKEN_TOTAL, TOPK), jnp.float32) ** steps_of(key_list[13], (TOKEN_TOTAL, TOPK), ((0, 256),), -0.2, 0.2)), 0.05, 1.0)
    return dict(query_rows=query_rows, key_rows=key_rows, value_rows=value_rows, gate_rows=gate_rows, log_decay=log_decay, head_gain=head_gain, out_weight=out_weight, residual=residual, ffn_gain=ffn_gain, gate_weight=gate_weight, up_weight=up_weight, down_weight=down_weight, routes=routes, route_weights=route_weights)


highest = lax.Precision.HIGHEST
rope_base = 10000.0
group_eps = 1e-05
square_eps = 1e-06
clamp_limit = 7.0
swish_alpha = 1.702

def rotary_angles(positions, head_dim):
    half_dim = head_dim // 2
    inverse = rope_base ** (-jnp.arange(half_dim, dtype=jnp.float32) / half_dim)
    return positions[:, None] * inverse[None, :]

def rotate(values, angles):
    half_dim = values.shape[-1] // 2
    cosine = jnp.cos(angles)[:, None, :]
    sine_table = jnp.sin(angles)[:, None, :]
    first_half = values[..., :half_dim]
    second_half = values[..., half_dim:]
    return jnp.concatenate([first_half * cosine - second_half * sine_table, second_half * cosine + first_half * sine_table], axis=-1)

def block_pass(carry_state, queries, keys_rot, values, log_step):
    length = queries.shape[0]
    cumulative = jnp.cumsum(log_step, axis=0)
    gap_matrix = cumulative[:, None, :] - cumulative[None, :, :]
    causal = jnp.arange(length, dtype=jnp.int32)[:, None] >= jnp.arange(length, dtype=jnp.int32)[None, :]
    weights = jnp.where(causal[:, :, None], jnp.exp(jnp.minimum(gap_matrix, 0.0)), 0.0)
    scores = jnp.einsum('ihd,jhd->ijh', queries, keys_rot, precision=highest) * weights
    inner_part = jnp.einsum('ijh,jhe->ihe', scores, values, precision=highest)
    cross_part = jnp.einsum('ihd,hde->ihe', queries, carry_state, precision=highest) * jnp.exp(cumulative)[:, :, None]
    total_log = cumulative[-1]
    tail_weight = jnp.exp(total_log[None, :] - cumulative)
    carried = carry_state * jnp.exp(total_log)[:, None, None] + jnp.einsum('jhd,jh,jhe->hde', keys_rot, tail_weight, values, precision=highest)
    return (carried, inner_part + cross_part)

def head_norm(retained, gain_row, gate_rows):
    mean_part = lax.optimization_barrier(jnp.mean(retained, axis=-1, keepdims=True))
    centred = retained - mean_part
    variance = lax.optimization_barrier(jnp.mean(centred * centred, axis=-1, keepdims=True))
    scaled = (centred * lax.rsqrt(variance + group_eps)).reshape(retained.shape[0], -1)
    return (scaled * gain_row * jax.nn.silu(gate_rows.astype(jnp.float32))).astype(jnp.bfloat16)

def square_norm(updated, gain_row):
    factor = lax.rsqrt(lax.optimization_barrier(jnp.mean(updated * updated, axis=-1, keepdims=True)) + square_eps)
    return (updated * factor * gain_row).astype(jnp.bfloat16)

def expert_rows(rows, gate_part, up_part):
    gate_pre = jnp.dot(rows, gate_part, preferred_element_type=jnp.float32)
    up_pre = jnp.dot(rows, up_part, preferred_element_type=jnp.float32)
    gate_clip = jnp.minimum(gate_pre, clamp_limit)
    up_clip = jnp.clip(up_pre, -clamp_limit, clamp_limit)
    return ((up_clip + 1.0) * (gate_clip * jax.nn.sigmoid(gate_clip * swish_alpha))).astype(jnp.bfloat16)

def slot_ranks(route_block, experts):
    flat_routes = route_block.reshape(-1)
    onehot = (flat_routes[:, None] == jnp.arange(experts, dtype=jnp.int32)[None, :]).astype(jnp.int32)
    return (flat_routes, lax.optimization_barrier(jnp.sum(jnp.cumsum(onehot, axis=0) * onehot, axis=1)) - 1)

def reference(query_rows, key_rows, value_rows, gate_rows, log_decay, head_gain, out_weight, residual, ffn_gain, gate_weight, up_weight, down_weight, routes, route_weights):
    positions = jnp.arange(TOKEN_TOTAL, dtype=jnp.float32)
    angles = rotary_angles(positions, HEAD_DIM)
    head_shape = (TOKEN_TOTAL, HEAD_TOTAL, HEAD_DIM)
    queries = rotate(query_rows.astype(jnp.float32).reshape(head_shape), angles)
    keys_rot = rotate(key_rows.astype(jnp.float32).reshape(head_shape), angles) * HEAD_DIM ** (-0.5)
    values = value_rows.astype(jnp.float32).reshape(head_shape)
    block_count = TOKEN_TOTAL // BLOCK

    def advance(carry_state, pieces):
        return block_pass(carry_state, pieces[0], pieces[1], pieces[2], pieces[3])
    start_state = jnp.zeros((HEAD_TOTAL, HEAD_DIM, HEAD_DIM), jnp.float32)
    block_shape = (block_count, BLOCK, HEAD_TOTAL, HEAD_DIM)
    _, retained = lax.scan(advance, start_state, (queries.reshape(block_shape), keys_rot.reshape(block_shape), values.reshape(block_shape), log_decay.reshape(block_count, BLOCK, HEAD_TOTAL)))
    retained = retained.reshape(head_shape)
    hidden = head_norm(retained, head_gain, gate_rows)
    updated = residual.astype(jnp.float32) + jnp.dot(hidden, out_weight, preferred_element_type=jnp.float32)
    ffn_in = square_norm(updated, ffn_gain)
    block_total = TOKEN_TOTAL // ROWS_DEV
    grouped = routes.reshape(block_total, ROWS_DEV, TOPK)
    flat_experts, flat_ranks = jax.vmap(partial(slot_ranks, experts=EXPERTS))(grouped)
    block_index = jnp.arange(block_total, dtype=jnp.int32)[:, None]
    slot_index = flat_experts * (block_total * CAP) + block_index * CAP + flat_ranks
    row_index = block_index * ROWS_DEV + jnp.arange(ROWS_DEV * TOPK, dtype=jnp.int32)[None, :] // TOPK
    source_row = jnp.full((EXPERTS * block_total * CAP,), TOKEN_TOTAL, jnp.int32).at[slot_index.reshape(-1)].set(row_index.reshape(-1))
    slot_weight = jnp.zeros((EXPERTS * block_total * CAP,), jnp.float32).at[slot_index.reshape(-1)].set(route_weights.reshape(-1))
    padded = jnp.concatenate([ffn_in, jnp.zeros((1, D), jnp.bfloat16)], axis=0)
    quarter = FF // N_TP

    def expert_step(accumulated, pieces):
        sources, weight_col, gate_part, up_part, down_part = pieces
        activity = expert_rows(padded[sources], gate_part, up_part)
        partials = jnp.einsum('mqf,qfd->qmd', activity.reshape(-1, N_TP, quarter).astype(jnp.float32), down_part.reshape(N_TP, quarter, D).astype(jnp.float32))
        rounded = lax.optimization_barrier(partials.astype(jnp.bfloat16)).astype(jnp.float32)
        expert_out = lax.optimization_barrier(jnp.sum(rounded, axis=0)).astype(jnp.bfloat16)
        return (accumulated.at[sources].add(weight_col[:, None] * expert_out.astype(jnp.float32)), None)
    start_sum = jnp.zeros((TOKEN_TOTAL + 1, D), jnp.float32)
    accumulated, _ = lax.scan(expert_step, start_sum, (source_row.reshape(EXPERTS, -1), slot_weight.reshape(EXPERTS, -1), gate_weight, up_weight, down_weight))
    return (updated + accumulated[:TOKEN_TOTAL]).astype(jnp.bfloat16)
```

```python
import functools
import math

import jax
import jax.numpy as jnp
import numpy as np
from jax import lax
from jax.experimental import pallas as pl
from jax.experimental.pallas import tpu as pltpu
from jax.sharding import Mesh
from jax.sharding import PartitionSpec as P


HEAD_DIM = 128
HALF = HEAD_DIM // 2
TOPK = 4
SP = ("z", "x", "c")
SP_TP = ("z", "x", "c", "tp")
CAP = 6
TILE = 8
WIDE = 128

rope_base = 10000.0
group_eps = 1e-05
square_eps = 1e-06
clamp_limit = 7.0
swish_alpha = 1.702

F32 = jnp.float32
BF16 = jnp.bfloat16


def dims(lhs, rhs):
    return (((lhs,), (rhs,)), ((), ()))


def dot(a, b, lhs=1, rhs=0):
    return lax.dot_general(a, b, dims(lhs, rhs), preferred_element_type=F32)


def iota(shape, dim):
    return lax.broadcasted_iota(jnp.int32, shape, dim)


def call(kernel, out_shape, *args, flops=0, smem=(), scratch=()):
    moved = sum(math.prod(a.shape) * a.dtype.itemsize for a in args)
    specs = [
        pl.BlockSpec(memory_space=pltpu.SMEM if i in smem else pltpu.VMEM)
        for i in range(len(args))
    ]
    multi = isinstance(out_shape, (list, tuple))
    outs = [pl.BlockSpec(memory_space=pltpu.VMEM)] * len(out_shape) if multi else pl.BlockSpec(memory_space=pltpu.VMEM)
    return pl.pallas_call(
        kernel,
        out_shape=out_shape,
        in_specs=specs,
        out_specs=outs,
        scratch_shapes=list(scratch),
        compiler_params=pltpu.CompilerParams(vmem_limit_bytes=56 * 1024 * 1024),
        cost_estimate=pl.CostEstimate(flops=flops, bytes_accessed=moved, transcendentals=0),
    )(*args)


def shape(dims_, kind=BF16):
    return jax.ShapeDtypeStruct(dims_, kind)


def three_parts(value):
    first = value.astype(BF16)
    rest = value - first.astype(F32)
    second = rest.astype(BF16)
    return first, second, (rest - second.astype(F32)).astype(BF16)


def tables(cos_ref, sin_ref, base_ref):
    cos_own, sin_own = cos_ref[...], sin_ref[...]
    cos_base, sin_base = base_ref[0:1, :], base_ref[1:2, :]
    cosine = cos_base * cos_own - sin_base * sin_own
    sine = sin_base * cos_own + cos_base * sin_own
    return cosine, jnp.where(iota(sine.shape, 1) < HALF, -sine, sine)


def turned(values, cosine, sine):
    return values * cosine + pltpu.roll(values, HALF, 1) * sine


def state_kernel(k_ref, v_ref, decay_ref, cos_ref, sin_ref, base_ref, out_ref):
    rows, heads = decay_ref.shape
    cosine, sine = tables(cos_ref, sin_ref, base_ref)
    lower = (iota((rows, rows), 0) >= iota((rows, rows), 1)).astype(BF16)
    cumulative = sum(dot(lower, part) for part in three_parts(decay_ref[...]))
    per_head = HEAD_DIM // TILE
    line = iota((TILE, HEAD_DIM), 0)
    for h in range(heads):
        cols = slice(h * HEAD_DIM, (h + 1) * HEAD_DIM)
        keys = turned(k_ref[:, cols].astype(F32), cosine, sine) * HEAD_DIM ** (-0.5)
        column = cumulative[:, h : h + 1]
        total = column[rows - 1 : rows, :]
        tail = keys * jnp.exp(total - column)
        state = dot(tail.astype(BF16), v_ref[:, cols], 0, 0)
        group = slice(h * per_head, (h + 1) * per_head)
        out_ref[group, 0:TILE, :] = state.reshape(per_head, TILE, HEAD_DIM).astype(BF16)
        first, second, third = [p.astype(F32) for p in three_parts(total)]
        note = jnp.where(line == 0, first, jnp.where(line == 1, second, jnp.where(line == 2, third, 0.0)))
        out_ref[group, TILE : 2 * TILE, :] = jnp.broadcast_to(
            note.astype(BF16)[None], (per_head, TILE, HEAD_DIM)
        )


def scan_kernel(in_ref, out_ref):
    state = jnp.zeros((TILE, HEAD_DIM), F32)
    for j in range(in_ref.shape[0]):
        out_ref[j] = state.astype(BF16)
        piece = in_ref[j].astype(F32)
        total = piece[TILE : TILE + 1] + piece[TILE + 1 : TILE + 2] + piece[TILE + 2 : TILE + 3]
        state = state * jnp.exp(total) + piece[0:TILE]


def inner_kernel(q_ref, k_ref, v_ref, decay_ref, cos_ref, sin_ref, base_ref, out_ref, lead_ref):
    rows, heads = decay_ref.shape
    cosine, sine = tables(cos_ref, sin_ref, base_ref)
    causal = iota((rows, rows), 0) >= iota((rows, rows), 1)
    lower = causal.astype(BF16)
    parts = three_parts(decay_ref[...])
    cumulative = sum(dot(lower, part) for part in parts)
    across = sum(dot(part, lower, 0, 1) for part in parts)
    for h in range(heads):
        cols = slice(h * HEAD_DIM, (h + 1) * HEAD_DIM)
        keys = turned(k_ref[:, cols].astype(F32), cosine, sine) * HEAD_DIM ** (-0.5)
        queries = turned(q_ref[:, cols].astype(F32), cosine, sine)
        column = cumulative[:, h : h + 1]
        gap = column - across[h : h + 1, :]
        weights = jnp.where(causal, jnp.exp(jnp.minimum(gap, 0.0)), 0.0)
        scores = dot(queries.astype(BF16), keys.astype(BF16), 1, 1) * weights
        out_ref[:, cols] = dot(scores.astype(BF16), v_ref[:, cols])
        lead_ref[:, cols] = (queries * jnp.exp(column)).astype(BF16)


def mix_kernel(inner_ref, lead_ref, enter_ref, gate_ref, gain_ref, weight_ref, out_ref, hidden_ref):
    heads = inner_ref.shape[1] // HEAD_DIM
    for h in range(heads):
        cols = slice(h * HEAD_DIM, (h + 1) * HEAD_DIM)
        kept = inner_ref[:, cols] + dot(lead_ref[:, cols], enter_ref[cols, :])
        centred = kept - jnp.mean(kept, axis=-1, keepdims=True)
        variance = jnp.mean(centred * centred, axis=-1, keepdims=True)
        gate = gate_ref[:, cols].astype(F32)
        opened = gate / (1.0 + jnp.exp(-gate))
        scaled = centred * lax.rsqrt(variance + group_eps)
        hidden_ref[:, cols] = (scaled * gain_ref[:, cols] * opened).astype(BF16)
    width = out_ref.shape[1]
    step = 512
    for n in range(0, width, step):
        out_ref[:, n : n + step] = dot(hidden_ref[...], weight_ref[:, n : n + step]).astype(BF16)


def norm_kernel(sum_ref, residual_ref, gain_ref, routes_ref, shares_ref, updated_ref, out_ref):
    updated = residual_ref[...].astype(F32)
    for i in range(sum_ref.shape[0]):
        updated = updated + sum_ref[i].astype(F32)
    updated_ref[...] = updated
    factor = lax.rsqrt(jnp.mean(updated * updated, axis=-1, keepdims=True) + square_eps)
    width = updated.shape[1]
    out_ref[:, 0:width] = (updated * factor * gain_ref[...]).astype(BF16)
    rows = updated.shape[0]
    lane = iota((rows, WIDE), 1)
    expert = lane % (WIDE // 2)
    table = jnp.zeros((rows, WIDE), F32)
    for k in range(TOPK):
        table = table + jnp.where(routes_ref[:, k : k + 1] == expert, shares_ref[:, k : k + 1], 0.0)
    first = table.astype(BF16).astype(F32)
    out_ref[:, width : width + WIDE] = jnp.where(lane < WIDE // 2, first, table - first).astype(BF16)


def lane_of(dest, place, half):
    return (dest // 2) * 8 + place * 2 + dest % 2 + half * (WIDE // 2)


def gather_kernel(place_ref, rows_ref, *out_refs):
    count = rows_ref.shape[0]
    width = rows_ref.shape[1] - WIDE
    block = count // 4
    dests = 16
    place = place_ref[0]
    table = rows_ref[:, width : width + WIDE]
    choose = (iota((dests, WIDE), 1) == lane_of(iota((dests, WIDE), 0), place, 0)).astype(BF16)
    named = (dot(choose, table, 1, 1) > 0.0).astype(F32)
    early, late = iota((count, count), 0), iota((count, count), 1)
    before = ((early < late) & (early // block == late // block)).astype(BF16)
    rank = dot(named.astype(BF16), before).astype(jnp.int32)
    slot = rank + CAP * (iota((dests, count), 1) // block)
    slot = jnp.where(named > 0.0, slot, -1)
    for c, out_ref in enumerate(out_refs):
        line = iota((dests, TILE, count), 1) + c * TILE
        pick = (slot[:, None, :] == line).astype(F32).reshape(dests * TILE, count).astype(BF16)
        step = 512
        for n in range(0, width, step):
            out_ref[:, n : n + step] = dot(pick, rows_ref[:, n : n + step]).astype(BF16)


def merge_kernel(place_ref, table_ref, *refs):
    back_refs, out_ref = refs[:-1], refs[-1]
    count = table_ref.shape[0]
    block = count // 4
    dests = 16
    place = place_ref[0]
    table = table_ref[...]
    high, low = [
        dot(table, (iota((WIDE, dests), 0) == lane_of(iota((WIDE, dests), 1), place, half)).astype(BF16))
        for half in (0, 1)
    ]
    late, early = iota((count, count), 0), iota((count, count), 1)
    before = ((early < late) & (early // block == late // block)).astype(BF16)
    rank = dot(before, (high > 0.0).astype(F32).astype(BF16))
    slot = rank + (CAP * (iota((count, dests), 0) // block)).astype(F32)
    spread = (iota((dests, dests * TILE), 1) // TILE == iota((dests, dests * TILE), 0)).astype(BF16)
    slot_wide = dot(slot.astype(BF16), spread).astype(jnp.int32)
    high_wide, low_wide = dot(high.astype(BF16), spread), dot(low.astype(BF16), spread)
    place_in = iota(slot_wide.shape, 1) % TILE
    mixes = []
    for c in range(len(back_refs)):
        here = slot_wide == place_in + c * TILE
        mixes.append(
            [jnp.where(here, part, 0.0).astype(BF16) for part in (high_wide, low_wide)]
        )
    width = out_ref.shape[1]
    step = 512
    for n in range(0, width, step):
        total = None
        for (first, second), back_ref in zip(mixes, back_refs):
            piece = back_ref[:, n : n + step]
            part = dot(first, piece) + dot(second, piece)
            total = part if total is None else total + part
        out_ref[:, n : n + step] = total.astype(BF16)


def expert_kernel(own_ref, right_ref, left_ref, far_r_ref, far_l_ref, gate_ref, up_ref, down_ref, *refs):
    outs, (all_ref, act_ref) = refs[:-2], refs[-2:]
    start = 0
    ranges = []
    for ref in (own_ref, right_ref, left_ref, far_r_ref, far_l_ref):
        rows = ref.shape[0]
        all_ref[start : start + rows, :] = ref[...]
        ranges.append((start, start + rows))
        start += rows
    hidden = gate_ref.shape[1]
    step = 256
    for n in range(0, hidden, step):
        cols = slice(n, n + step)
        gate = jnp.minimum(dot(all_ref[...], gate_ref[:, cols]), clamp_limit)
        up = jnp.clip(dot(all_ref[...], up_ref[:, cols]), -clamp_limit, clamp_limit)
        act_ref[:, cols] = ((up + 1.0) * (gate / (1.0 + jnp.exp(-swish_alpha * gate)))).astype(BF16)
    width = down_ref.shape[1]
    for n in range(0, width, 512):
        cols = slice(n, n + 512)
        part = dot(act_ref[...], down_ref[:, cols]).astype(BF16)
        for (low, high), out_ref in zip(ranges, outs):
            out_ref[:, cols] = part[low:high]


def ring(size, shift):
    return [(i, (i + shift) % size) for i in range(size)]


def add(a, b):
    return (a.astype(F32) + b.astype(F32)).astype(BF16)


def body(
    query_rows,
    key_rows,
    value_rows,
    gate_rows,
    log_decay,
    head_gain,
    out_weight,
    residual,
    ffn_gain,
    gate_weight,
    up_weight,
    down_weight,
    routes,
    route_weights,
):
    tok_count, heads = log_decay.shape
    local = heads * HEAD_DIM
    rows_own, width = residual.shape
    sp_count = lax.axis_size(SP)
    tp_count = lax.axis_size("tp")
    sp_index = lax.axis_index(SP)

    inverse = rope_base ** (-np.arange(HALF, dtype=np.float64) / HALF)
    inverse = np.concatenate([inverse, inverse])
    inside = np.arange(tok_count, dtype=np.float64)[:, None] * inverse[None]
    starts = (np.arange(sp_count, dtype=np.float64) * tok_count)[:, None] * inverse[None]
    cos_own, sin_own = jnp.asarray(np.cos(inside), F32), jnp.asarray(np.sin(inside), F32)
    base_all = jnp.asarray(np.stack([np.cos(starts), np.sin(starts)], axis=1), F32)
    base = lax.dynamic_index_in_dim(base_all, sp_index, 0, keepdims=False)

    message = call(
        state_kernel,
        shape((sp_count, 2 * TILE, HEAD_DIM)),
        key_rows, value_rows, log_decay, cos_own, sin_own, base,
        flops=2 * tok_count * local * HEAD_DIM,
    )
    spans = lax.all_to_all(message, SP, 0, 0, tiled=True)
    inner, lead = call(
        inner_kernel,
        [shape((tok_count, local), F32), shape((tok_count, local))],
        query_rows, key_rows, value_rows, log_decay, cos_own, sin_own, base,
        flops=4 * tok_count * tok_count * local,
    )
    entering = call(scan_kernel, shape((sp_count, TILE, HEAD_DIM)), spans)
    entering = lax.all_to_all(entering, SP, 0, 0, tiled=True).reshape(local, HEAD_DIM)
    mixed = call(
        mix_kernel,
        shape((tok_count, width)),
        inner, lead, entering, gate_rows, head_gain.reshape(1, local), out_weight,
        flops=2 * tok_count * local * width,
        scratch=[pltpu.VMEM((tok_count, local), BF16)],
    )
    pieces = lax.all_to_all(mixed.reshape(tp_count, rows_own, width), "tp", 0, 0, tiled=True)
    own_routes = lax.dynamic_slice_in_dim(routes, lax.axis_index("tp") * rows_own, rows_own, 0)
    updated, extended = call(
        norm_kernel,
        [shape((rows_own, width), F32), shape((rows_own, width + WIDE))],
        pieces, residual, ffn_gain.reshape(1, width), own_routes, route_weights,
    )

    place = lax.axis_index("x").astype(jnp.int32).reshape(1)
    x_count = lax.axis_size("x")
    spread = jnp.broadcast_to(extended[None], (x_count, rows_own, width + WIDE))
    near = lax.all_to_all(spread, "x", 0, 0, tiled=True).reshape(x_count * rows_own, width + WIDE)
    dests = sp_count // x_count
    chunks = x_count * CAP // TILE
    outgoing = call(
        gather_kernel,
        [shape((dests * TILE, width))] * chunks,
        place, near,
        flops=2 * chunks * dests * TILE * near.shape[0] * width,
        smem=(0,),
    )
    gate_part, up_part, down_part = gate_weight[0], up_weight[0], down_weight[0]
    ahead, behind = ring(tp_count, 1), ring(tp_count, -1)
    returned = []
    for piece in outgoing:
        own = lax.all_to_all(piece.reshape(dests, TILE, width), ("z", "c"), 0, 0, tiled=True)
        own = own.reshape(dests * TILE, width)
        rows = own.shape[0]
        half = rows // 2
        right = lax.ppermute(own, "tp", ahead)
        left = lax.ppermute(own, "tp", behind)
        far_r = lax.ppermute(right[:half], "tp", ahead)
        far_l = lax.ppermute(left[half:], "tp", behind)
        out_own, out_right, out_left, out_far_r, out_far_l = call(
            expert_kernel,
            [shape((rows, width))] * 3 + [shape((half, width))] * 2,
            own, right, left, far_r, far_l, gate_part, up_part, down_part,
            flops=6 * 4 * rows * width * gate_part.shape[1],
            scratch=[pltpu.VMEM((4 * rows, width), BF16), pltpu.VMEM((4 * rows, gate_part.shape[1]), BF16)],
        )
        via_r = lax.ppermute(out_far_r, "tp", behind)
        via_l = lax.ppermute(out_far_l, "tp", ahead)
        send_r = jnp.concatenate([add(out_right[:half], via_r), out_right[half:]], axis=0)
        send_l = jnp.concatenate([out_left[:half], add(out_left[half:], via_l)], axis=0)
        back_r = lax.ppermute(send_r, "tp", behind)
        back_l = lax.ppermute(send_l, "tp", ahead)
        total = (out_own.astype(F32) + back_r.astype(F32) + back_l.astype(F32)).astype(BF16)
        back = lax.all_to_all(total.reshape(dests, TILE, width), ("z", "c"), 0, 0, tiled=True)
        returned.append(back.reshape(dests * TILE, width))
    merged = call(
        merge_kernel,
        shape((x_count * rows_own, width)),
        place, near[:, width:], *returned,
        flops=4 * chunks * dests * TILE * near.shape[0] * width,
        smem=(0,),
    )
    parts = lax.all_to_all(merged.reshape(x_count, rows_own, width), "x", 0, 0, tiled=True)
    return (updated + jnp.sum(parts.astype(F32), axis=0)).astype(BF16)


def solution(mesh):
    finer = Mesh(mesh.devices.reshape(8, 4, 2, mesh.shape["tp"]), SP_TP)
    return jax.shard_map(
        body,
        mesh=finer,
        in_specs=(
            P(SP, "tp"),
            P(SP, "tp"),
            P(SP, "tp"),
            P(SP, "tp"),
            P(SP, "tp"),
            P("tp"),
            P("tp", None),
            P(SP_TP, None),
            P(),
            P(SP, None, "tp"),
            P(SP, None, "tp"),
            P(SP, "tp", None),
            P(SP, None),
            P(SP_TP, None),
        ),
        out_specs=P(SP_TP, None),
        check_vma=False,
    )
```

```python
import math

import jax
import jax.numpy as jnp
import numpy as np
from jax import lax
from jax.experimental import pallas as pl
from jax.experimental.pallas import tpu as pltpu
from jax.sharding import Mesh
from jax.sharding import PartitionSpec as P


HEAD_DIM = 128
HALF = HEAD_DIM // 2
TOPK = 4
SP = ("z", "x", "c")
SP_TP = ("z", "x", "c", "tp")
CAP = 6
TILE = 8
WIDE = 128

rope_base = 10000.0
group_eps = 1e-05
square_eps = 1e-06
clamp_limit = 7.0
swish_alpha = 1.702

F32 = jnp.float32
BF16 = jnp.bfloat16


def dims(lhs, rhs):
    return (((lhs,), (rhs,)), ((), ()))


def dot(a, b, lhs=1, rhs=0):
    return lax.dot_general(a, b, dims(lhs, rhs), preferred_element_type=F32)


def iota(shape, dim):
    return lax.broadcasted_iota(jnp.int32, shape, dim)


def call(kernel, out_shape, *args, flops=0, smem=(), scratch=()):
    moved = sum(math.prod(a.shape) * a.dtype.itemsize for a in args)
    specs = [
        pl.BlockSpec(memory_space=pltpu.SMEM if i in smem else pltpu.VMEM)
        for i in range(len(args))
    ]
    multi = isinstance(out_shape, (list, tuple))
    outs = [pl.BlockSpec(memory_space=pltpu.VMEM)] * len(out_shape) if multi else pl.BlockSpec(memory_space=pltpu.VMEM)
    return pl.pallas_call(
        kernel,
        out_shape=out_shape,
        in_specs=specs,
        out_specs=outs,
        scratch_shapes=list(scratch),
        compiler_params=pltpu.CompilerParams(vmem_limit_bytes=56 * 1024 * 1024),
        cost_estimate=pl.CostEstimate(flops=flops, bytes_accessed=moved, transcendentals=0),
    )(*args)


def shape(dims_, kind=BF16):
    return jax.ShapeDtypeStruct(dims_, kind)


def three_parts(value):
    first = value.astype(BF16)
    rest = value - first.astype(F32)
    second = rest.astype(BF16)
    return first, second, (rest - second.astype(F32)).astype(BF16)


def tables(cos_ref, sin_ref, base_ref):
    cos_own, sin_own = cos_ref[...], sin_ref[...]
    cos_base, sin_base = base_ref[0:1, :], base_ref[1:2, :]
    cosine = cos_base * cos_own - sin_base * sin_own
    sine = sin_base * cos_own + cos_base * sin_own
    return cosine, jnp.where(iota(sine.shape, 1) < HALF, -sine, sine)


def turned(values, cosine, sine):
    return values * cosine + pltpu.roll(values, HALF, 1) * sine


def state_kernel(k_ref, v_ref, decay_ref, cos_ref, sin_ref, base_ref, out_ref):
    rows, heads = decay_ref.shape
    cosine, sine = tables(cos_ref, sin_ref, base_ref)
    lower = (iota((rows, rows), 0) >= iota((rows, rows), 1)).astype(BF16)
    cumulative = sum(dot(lower, part) for part in three_parts(decay_ref[...]))
    share = out_ref.shape[1] - TILE
    per_head = HEAD_DIM // share
    for h in range(heads):
        cols = slice(h * HEAD_DIM, (h + 1) * HEAD_DIM)
        keys = turned(k_ref[:, cols].astype(F32), cosine, sine) * HEAD_DIM ** (-0.5)
        column = cumulative[:, h : h + 1]
        total = column[rows - 1 : rows, :]
        tail = keys * jnp.exp(total - column)
        state = dot(tail.astype(BF16), v_ref[:, cols], 0, 0)
        for i in range(per_head):
            out_ref[h * per_head + i, 0:share, :] = state[i * share : (i + 1) * share].astype(BF16)
            out_ref[h * per_head + i, share : share + TILE, :] = note_of(total)


def note_of(total):
    line = iota((TILE, HEAD_DIM), 0)
    first, second, third = [p.astype(F32) for p in three_parts(total)]
    note = jnp.where(line == 0, first, jnp.where(line == 1, second, jnp.where(line == 2, third, 0.0)))
    return note.astype(BF16)


def total_of(note):
    return note[0:1] + note[1:2] + note[2:3]


def group_kernel(in_ref, before_ref, reach_ref, out_ref):
    share = in_ref.shape[1] - TILE
    state = jnp.zeros((share, HEAD_DIM), F32)
    reach = jnp.zeros((1, HEAD_DIM), F32)
    for j in range(in_ref.shape[0]):
        before_ref[j] = state
        reach_ref[j] = jnp.broadcast_to(reach, (TILE, HEAD_DIM))
        piece = in_ref[j].astype(F32)
        total = total_of(piece[share:])
        state = state * jnp.exp(total) + piece[:share]
        reach = reach + total
    for i in range(out_ref.shape[0]):
        out_ref[i, 0:share, :] = state.astype(BF16)
        out_ref[i, share:, :] = note_of(reach)


def enter_kernel(place_ref, in_ref, before_ref, reach_ref, out_ref):
    share = out_ref.shape[1]
    place = place_ref[0]
    state = jnp.zeros((share, HEAD_DIM), F32)
    for j in range(in_ref.shape[0]):
        piece = in_ref[j].astype(F32)
        later = state * jnp.exp(total_of(piece[share:])) + piece[:share]
        state = jnp.where(j < place, later, state)
    for j in range(out_ref.shape[0]):
        out_ref[j] = (state * jnp.exp(reach_ref[j, 0:1]) + before_ref[j]).astype(BF16)


def inner_kernel(q_ref, k_ref, v_ref, decay_ref, cos_ref, sin_ref, base_ref, out_ref, lead_ref):
    rows, heads = decay_ref.shape
    cosine, sine = tables(cos_ref, sin_ref, base_ref)
    causal = iota((rows, rows), 0) >= iota((rows, rows), 1)
    lower = causal.astype(BF16)
    parts = three_parts(decay_ref[...])
    cumulative = sum(dot(lower, part) for part in parts)
    across = sum(dot(part, lower, 0, 1) for part in parts)
    for h in range(heads):
        cols = slice(h * HEAD_DIM, (h + 1) * HEAD_DIM)
        keys = turned(k_ref[:, cols].astype(F32), cosine, sine) * HEAD_DIM ** (-0.5)
        queries = turned(q_ref[:, cols].astype(F32), cosine, sine)
        column = cumulative[:, h : h + 1]
        gap = column - across[h : h + 1, :]
        weights = jnp.where(causal, jnp.exp(jnp.minimum(gap, 0.0)), 0.0)
        scores = dot(queries.astype(BF16), keys.astype(BF16), 1, 1) * weights
        out_ref[:, cols] = dot(scores.astype(BF16), v_ref[:, cols])
        lead_ref[:, cols] = (queries * jnp.exp(column)).astype(BF16)


def mix_kernel(inner_ref, lead_ref, enter_ref, gate_ref, gain_ref, weight_ref, out_ref, hidden_ref):
    heads = inner_ref.shape[1] // HEAD_DIM
    for h in range(heads):
        cols = slice(h * HEAD_DIM, (h + 1) * HEAD_DIM)
        kept = inner_ref[:, cols] + dot(lead_ref[:, cols], enter_ref[cols, :])
        centred = kept - jnp.mean(kept, axis=-1, keepdims=True)
        variance = jnp.mean(centred * centred, axis=-1, keepdims=True)
        gate = gate_ref[:, cols].astype(F32)
        opened = gate / (1.0 + jnp.exp(-gate))
        scaled = centred * lax.rsqrt(variance + group_eps)
        hidden_ref[:, cols] = (scaled * gain_ref[:, cols] * opened).astype(BF16)
    step = 512

    @pl.loop(0, out_ref.shape[1] // step)
    def _(n):
        cols = pl.ds(pl.multiple_of(n * step, step), step)
        out_ref[:, cols] = dot(hidden_ref[...], weight_ref[:, cols]).astype(BF16)


def norm_kernel(sum_ref, residual_ref, gain_ref, routes_ref, shares_ref, updated_ref, out_ref):
    updated = residual_ref[...].astype(F32)
    for i in range(sum_ref.shape[0]):
        updated = updated + sum_ref[i].astype(F32)
    updated_ref[...] = updated
    factor = lax.rsqrt(jnp.mean(updated * updated, axis=-1, keepdims=True) + square_eps)
    width = updated.shape[1]
    scaled = (updated * factor * gain_ref[...]).astype(BF16)
    rows = updated.shape[0]
    lane = iota((rows, WIDE), 1)
    expert = lane % (WIDE // 2)
    table = jnp.zeros((rows, WIDE), F32)
    for k in range(TOPK):
        table = table + jnp.where(routes_ref[:, k : k + 1] == expert, shares_ref[:, k : k + 1], 0.0)
    first = table.astype(BF16).astype(F32)
    noted = jnp.where(lane < WIDE // 2, first, table - first).astype(BF16)
    for i in range(out_ref.shape[0]):
        out_ref[i, :, 0:width] = scaled
        out_ref[i, :, width : width + WIDE] = noted


def lane_of(dest, place, half):
    return (dest // 2) * 8 + place * 2 + dest % 2 + half * (WIDE // 2)


def gather_kernel(place_ref, rows_ref, *refs):
    out_refs, pick_ref = refs[:-1], refs[-1]
    count = rows_ref.shape[0]
    width = rows_ref.shape[1] - WIDE
    block = count // 4
    dests = 16
    place = place_ref[0]
    table = rows_ref[:, width : width + WIDE]
    choose = (iota((dests, WIDE), 1) == lane_of(iota((dests, WIDE), 0), place, 0)).astype(BF16)
    named = (dot(choose, table, 1, 1) > 0.0).astype(F32)
    early, late = iota((count, count), 0), iota((count, count), 1)
    before = ((early < late) & (early // block == late // block)).astype(BF16)
    rank = dot(named.astype(BF16), before).astype(jnp.int32)
    slot = rank + CAP * (iota((dests, count), 1) // block)
    slot = jnp.where(named > 0.0, slot, -1)
    for c, out_ref in enumerate(out_refs):
        line = iota((dests, TILE, count), 1) + c * TILE
        pick = (slot[:, None, :] == line).astype(F32).reshape(dests * TILE, count).astype(BF16)
        pick_ref[c * dests * TILE : (c + 1) * dests * TILE, :] = pick
    step = 256

    @pl.loop(0, width // step)
    def _(n):
        cols = pl.ds(pl.multiple_of(n * step, step), step)
        chosen = dot(pick_ref[...], rows_ref[:, cols]).astype(BF16)
        for c, out_ref in enumerate(out_refs):
            out_ref[:, cols] = chosen[c * dests * TILE : (c + 1) * dests * TILE]


def merge_kernel(place_ref, table_ref, *refs):
    back_refs, out_ref, mix_refs = refs[:-3], refs[-3], refs[-2:]
    count = table_ref.shape[0]
    block = count // 4
    dests = 16
    place = place_ref[0]
    table = table_ref[...]
    high, low = [
        dot(table, (iota((WIDE, dests), 0) == lane_of(iota((WIDE, dests), 1), place, half)).astype(BF16))
        for half in (0, 1)
    ]
    late, early = iota((count, count), 0), iota((count, count), 1)
    before = ((early < late) & (early // block == late // block)).astype(BF16)
    rank = dot(before, (high > 0.0).astype(F32).astype(BF16))
    slot = rank + (CAP * (iota((count, dests), 0) // block)).astype(F32)
    spread = (iota((dests, dests * TILE), 1) // TILE == iota((dests, dests * TILE), 0)).astype(BF16)
    slot_wide = dot(slot.astype(BF16), spread).astype(jnp.int32)
    high_wide, low_wide = dot(high.astype(BF16), spread), dot(low.astype(BF16), spread)
    place_in = iota(slot_wide.shape, 1) % TILE
    high_ref, low_ref = mix_refs
    span = dests * TILE
    for c in range(len(back_refs)):
        here = slot_wide == place_in + c * TILE
        high_ref[:, c * span : (c + 1) * span] = jnp.where(here, high_wide, 0.0).astype(BF16)
        low_ref[:, c * span : (c + 1) * span] = jnp.where(here, low_wide, 0.0).astype(BF16)
    step = 256

    @pl.loop(0, out_ref.shape[1] // step)
    def _(n):
        cols = pl.ds(pl.multiple_of(n * step, step), step)
        piece = jnp.concatenate([ref[:, cols] for ref in back_refs], axis=0)
        out_ref[:, cols] = (dot(high_ref[...], piece) + dot(low_ref[...], piece)).astype(BF16)


def expert_kernel(own_ref, right_ref, left_ref, far_ref, gate_ref, up_ref, down_ref, *refs):
    outs, (all_ref, act_ref) = refs[:-2], refs[-2:]
    rows = own_ref.shape[0]
    for i, ref in enumerate((own_ref, right_ref, left_ref, far_ref)):
        all_ref[i * rows : (i + 1) * rows, :] = ref[...]
    step = 256

    @pl.loop(0, gate_ref.shape[1] // step)
    def _(n):
        cols = pl.ds(pl.multiple_of(n * step, step), step)
        gate = jnp.minimum(dot(all_ref[...], gate_ref[:, cols]), clamp_limit)
        up = jnp.clip(dot(all_ref[...], up_ref[:, cols]), -clamp_limit, clamp_limit)
        act_ref[:, cols] = ((up + 1.0) * (gate / (1.0 + jnp.exp(-swish_alpha * gate)))).astype(BF16)

    @pl.loop(0, down_ref.shape[1] // step)
    def _(n):
        cols = pl.ds(pl.multiple_of(n * step, step), step)
        part = dot(act_ref[...], down_ref[:, cols]).astype(BF16)
        for i, out_ref in enumerate(outs):
            out_ref[:, cols] = part[i * rows : (i + 1) * rows]


def ring(size, shift):
    return [(i, (i + shift) % size) for i in range(size)]


def add(a, b):
    return (a.astype(F32) + b.astype(F32)).astype(BF16)


def body(
    query_rows,
    key_rows,
    value_rows,
    gate_rows,
    log_decay,
    head_gain,
    out_weight,
    residual,
    ffn_gain,
    gate_weight,
    up_weight,
    down_weight,
    routes,
    route_weights,
):
    tok_count, heads = log_decay.shape
    local = heads * HEAD_DIM
    rows_own, width = residual.shape
    sp_count = lax.axis_size(SP)
    tp_count = lax.axis_size("tp")
    sp_index = lax.axis_index(SP)

    inverse = rope_base ** (-np.arange(HALF, dtype=np.float64) / HALF)
    inverse = np.concatenate([inverse, inverse])
    inside = np.arange(tok_count, dtype=np.float64)[:, None] * inverse[None]
    starts = (np.arange(sp_count, dtype=np.float64) * tok_count)[:, None] * inverse[None]
    cos_own, sin_own = jnp.asarray(np.cos(inside), F32), jnp.asarray(np.sin(inside), F32)
    base_all = jnp.asarray(np.stack([np.cos(starts), np.sin(starts)], axis=1), F32)
    base = lax.dynamic_index_in_dim(base_all, sp_index, 0, keepdims=False)

    near_count = lax.axis_size(("x", "c"))
    far_count = lax.axis_size("z")
    share = local // near_count
    message = call(
        state_kernel,
        shape((near_count, share + TILE, HEAD_DIM)),
        key_rows, value_rows, log_decay, cos_own, sin_own, base,
        flops=2 * tok_count * local * HEAD_DIM,
    )
    spans = lax.all_to_all(message, ("x", "c"), 0, 0, tiled=True)
    inner, lead = call(
        inner_kernel,
        [shape((tok_count, local), F32), shape((tok_count, local))],
        query_rows, key_rows, value_rows, log_decay, cos_own, sin_own, base,
        flops=4 * tok_count * tok_count * local,
    )
    before, reach, group = call(
        group_kernel,
        [shape((near_count, share, HEAD_DIM), F32), shape((near_count, TILE, HEAD_DIM), F32), shape((far_count, share + TILE, HEAD_DIM))],
        spans,
    )
    groups = lax.all_to_all(group, "z", 0, 0, tiled=True)
    entering = call(
        enter_kernel,
        shape((near_count, share, HEAD_DIM)),
        lax.axis_index("z").astype(jnp.int32).reshape(1), groups, before, reach,
        smem=(0,),
    )
    entering = lax.all_to_all(entering, ("x", "c"), 0, 0, tiled=True).reshape(local, HEAD_DIM)
    mixed = call(
        mix_kernel,
        shape((tok_count, width)),
        inner, lead, entering, gate_rows, head_gain.reshape(1, local), out_weight,
        flops=2 * tok_count * local * width,
        scratch=[pltpu.VMEM((tok_count, local), BF16)],
    )
    pieces = lax.all_to_all(mixed.reshape(tp_count, rows_own, width), "tp", 0, 0, tiled=True)
    own_routes = lax.dynamic_slice_in_dim(routes, lax.axis_index("tp") * rows_own, rows_own, 0)
    x_count = lax.axis_size("x")
    updated, spread = call(
        norm_kernel,
        [shape((rows_own, width), F32), shape((x_count, rows_own, width + WIDE))],
        pieces, residual, ffn_gain.reshape(1, width), own_routes, route_weights,
    )

    place = lax.axis_index("x").astype(jnp.int32).reshape(1)
    near = lax.all_to_all(spread, "x", 0, 0, tiled=True).reshape(x_count * rows_own, width + WIDE)
    dests = sp_count // x_count
    chunks = x_count * CAP // TILE
    outgoing = call(
        gather_kernel,
        [shape((dests * TILE, width))] * chunks,
        place, near,
        flops=2 * chunks * dests * TILE * near.shape[0] * width,
        smem=(0,),
        scratch=[pltpu.VMEM((chunks * dests * TILE, near.shape[0]), BF16)],
    )
    gate_part, up_part, down_part = gate_weight[0], up_weight[0], down_weight[0]
    ahead, behind = ring(tp_count, 1), ring(tp_count, -1)
    returned = []
    for c, piece in enumerate(outgoing, 1):
        first, second = (ahead, behind) if c % 2 else (behind, ahead)
        own = lax.all_to_all(piece.reshape(dests, TILE, width), ("z", "c"), 0, 0, tiled=True)
        own = own.reshape(dests * TILE, width)
        rows = own.shape[0]
        one = lax.ppermute(own, "tp", first)
        two = lax.ppermute(own, "tp", second)
        far = lax.ppermute(one, "tp", first)
        out_own, out_one, out_two, out_far = call(
            expert_kernel,
            [shape((rows, width))] * 4,
            own, one, two, far, gate_part, up_part, down_part,
            flops=6 * 4 * rows * width * gate_part.shape[1],
            scratch=[pltpu.VMEM((4 * rows, width), BF16), pltpu.VMEM((4 * rows, gate_part.shape[1]), BF16)],
        )
        via = lax.ppermute(out_far, "tp", second)
        back_one = lax.ppermute(add(out_one, via), "tp", second)
        back_two = lax.ppermute(out_two, "tp", first)
        total = (out_own.astype(F32) + back_one.astype(F32) + back_two.astype(F32)).astype(BF16)
        back = lax.all_to_all(total.reshape(dests, TILE, width), ("z", "c"), 0, 0, tiled=True)
        returned.append(back.reshape(dests * TILE, width))
    merged = call(
        merge_kernel,
        shape((x_count * rows_own, width)),
        place, near[:, width:], *returned,
        flops=4 * chunks * dests * TILE * near.shape[0] * width,
        smem=(0,),
        scratch=[pltpu.VMEM((near.shape[0], chunks * dests * TILE), BF16)] * 2,
    )
    parts = lax.all_to_all(merged.reshape(x_count, rows_own, width), "x", 0, 0, tiled=True)
    return (updated + jnp.sum(parts.astype(F32), axis=0)).astype(BF16)


def solution(mesh):
    finer = Mesh(mesh.devices.reshape(8, 4, 2, mesh.shape["tp"]), SP_TP)
    return jax.shard_map(
        body,
        mesh=finer,
        in_specs=(
            P(SP, "tp"),
            P(SP, "tp"),
            P(SP, "tp"),
            P(SP, "tp"),
            P(SP, "tp"),
            P("tp"),
            P("tp", None),
            P(SP_TP, None),
            P(),
            P(SP, None, "tp"),
            P(SP, None, "tp"),
            P(SP, "tp", None),
            P(SP, None),
            P(SP_TP, None),
        ),
        out_specs=P(SP_TP, None),
        check_vma=False,
    )
```

```python
import functools
import math

import jax
import jax.numpy as jnp
import numpy as np
from jax import lax
from jax.experimental import pallas as pl
from jax.experimental.pallas import tpu as pltpu
from jax.sharding import Mesh
from jax.sharding import PartitionSpec as P


HEAD_DIM = 128
HALF = HEAD_DIM // 2
TOPK = 4
SP = ("z", "x", "c")
SP_TP = ("z", "x", "c", "tp")
CAP = 6
TILE = 8
WIDE = 128
PIECES = 2

rope_base = 10000.0
group_eps = 1e-05
square_eps = 1e-06
clamp_limit = 7.0
swish_alpha = 1.702

F32 = jnp.float32
BF16 = jnp.bfloat16


def dims(lhs, rhs):
    return (((lhs,), (rhs,)), ((), ()))


def dot(a, b, lhs=1, rhs=0):
    return lax.dot_general(a, b, dims(lhs, rhs), preferred_element_type=F32)


def iota(shape, dim):
    return lax.broadcasted_iota(jnp.int32, shape, dim)


def call(kernel, out_shape, *args, flops=0, smem=(), far=(), scratch=(), room=24):
    moved = sum(math.prod(a.shape) * a.dtype.itemsize for a in args)
    specs = [
        pl.BlockSpec(memory_space=pltpu.SMEM if i in smem else pltpu.HBM if i in far else pltpu.VMEM)
        for i in range(len(args))
    ]
    multi = isinstance(out_shape, (list, tuple))
    outs = [pl.BlockSpec(memory_space=pltpu.VMEM)] * len(out_shape) if multi else pl.BlockSpec(memory_space=pltpu.VMEM)
    return pl.pallas_call(
        kernel,
        out_shape=out_shape,
        in_specs=specs,
        out_specs=outs,
        scratch_shapes=list(scratch),
        compiler_params=pltpu.CompilerParams(vmem_limit_bytes=room * 1024 * 1024),
        cost_estimate=pl.CostEstimate(flops=flops, bytes_accessed=moved, transcendentals=0),
    )(*args)


def shape(dims_, kind=BF16):
    return jax.ShapeDtypeStruct(dims_, kind)


def three_parts(value):
    first = value.astype(BF16)
    rest = value - first.astype(F32)
    second = rest.astype(BF16)
    return first, second, (rest - second.astype(F32)).astype(BF16)


def tables(cos_ref, sin_ref, base_ref):
    cos_own, sin_own = [jnp.concatenate([ref[...]] * 2, axis=1) for ref in (cos_ref, sin_ref)]
    cos_base, sin_base = base_ref[0:1, :], base_ref[1:2, :]
    cosine = cos_base * cos_own - sin_base * sin_own
    sine = sin_base * cos_own + cos_base * sin_own
    return cosine, jnp.where(iota(sine.shape, 1) < HALF, -sine, sine)


def turned(values, cosine, sine):
    return values * cosine + pltpu.roll(values, HALF, 1) * sine


def state_kernel(k_ref, v_ref, decay_ref, cos_ref, sin_ref, base_ref, out_ref):
    rows, heads = decay_ref.shape
    cosine, sine = tables(cos_ref, sin_ref, base_ref)
    lower = (iota((rows, rows), 0) >= iota((rows, rows), 1)).astype(BF16)
    cumulative = sum(dot(lower, part) for part in three_parts(decay_ref[...]))
    share = out_ref.shape[1] - TILE
    per_head = HEAD_DIM // share
    for h in range(heads):
        cols = slice(h * HEAD_DIM, (h + 1) * HEAD_DIM)
        keys = turned(k_ref[:, cols].astype(F32), cosine, sine) * HEAD_DIM ** (-0.5)
        column = cumulative[:, h : h + 1]
        total = column[rows - 1 : rows, :]
        tail = keys * jnp.exp(total - column)
        state = dot(tail.astype(BF16), v_ref[:, cols], 0, 0)
        for i in range(per_head):
            out_ref[h * per_head + i, 0:share, :] = state[i * share : (i + 1) * share].astype(BF16)
            out_ref[h * per_head + i, share : share + TILE, :] = note_of(total)


def note_of(total):
    line = iota((TILE, HEAD_DIM), 0)
    first, second, third = [p.astype(F32) for p in three_parts(total)]
    note = jnp.where(line == 0, first, jnp.where(line == 1, second, jnp.where(line == 2, third, 0.0)))
    return note.astype(BF16)


def total_of(note):
    return note[0:1] + note[1:2] + note[2:3]


def group_kernel(in_ref, before_ref, reach_ref, out_ref):
    share = in_ref.shape[1] - TILE
    state = jnp.zeros((share, HEAD_DIM), F32)
    reach = jnp.zeros((1, HEAD_DIM), F32)
    for j in range(in_ref.shape[0]):
        before_ref[j] = state
        reach_ref[j] = jnp.broadcast_to(reach, (TILE, HEAD_DIM))
        piece = in_ref[j].astype(F32)
        total = total_of(piece[share:])
        state = state * jnp.exp(total) + piece[:share]
        reach = reach + total
    for i in range(out_ref.shape[0]):
        out_ref[i, 0:share, :] = state.astype(BF16)
        out_ref[i, share:, :] = note_of(reach)


def enter_kernel(place_ref, in_ref, before_ref, reach_ref, out_ref):
    share = out_ref.shape[1]
    place = place_ref[0]
    state = jnp.zeros((share, HEAD_DIM), F32)
    for j in range(in_ref.shape[0]):
        piece = in_ref[j].astype(F32)
        later = state * jnp.exp(total_of(piece[share:])) + piece[:share]
        state = jnp.where(j < place, later, state)
    for j in range(out_ref.shape[0]):
        out_ref[j] = (state * jnp.exp(reach_ref[j, 0:1]) + before_ref[j]).astype(BF16)


def inner_kernel(q_ref, k_ref, v_ref, decay_ref, cos_ref, sin_ref, base_ref, out_ref, lead_ref, across_ref):
    rows, heads = decay_ref.shape
    cosine, sine = tables(cos_ref, sin_ref, base_ref)
    causal = iota((rows, rows), 0) >= iota((rows, rows), 1)
    lower = causal.astype(BF16)
    parts = three_parts(decay_ref[...])
    cumulative = sum(dot(lower, part) for part in parts)
    across = sum(dot(part, lower, 0, 1) for part in parts)
    across_ref[...] = across
    lane = iota((rows, heads), 1)

    @pl.loop(0, heads)
    def _(h):
        cols = pl.ds(pl.multiple_of(h * HEAD_DIM, HEAD_DIM), HEAD_DIM)
        keys = turned(k_ref[:, cols].astype(F32), cosine, sine) * HEAD_DIM ** (-0.5)
        queries = turned(q_ref[:, cols].astype(F32), cosine, sine)
        column = jnp.sum(jnp.where(lane == h, cumulative, 0.0), axis=1, keepdims=True)
        gap = column - across_ref[pl.ds(h, 1), :]
        weights = jnp.where(causal, jnp.exp(jnp.minimum(gap, 0.0)), 0.0)
        scores = dot(queries.astype(BF16), keys.astype(BF16), 1, 1) * weights
        out_ref[:, cols] = dot(scores.astype(BF16), v_ref[:, cols])
        lead_ref[:, cols] = (queries * jnp.exp(column)).astype(BF16)


def mix_kernel(inner_ref, lead_ref, enter_ref, gate_ref, gain_ref, weight_ref, out_ref, hidden_ref):
    @pl.loop(0, inner_ref.shape[1] // HEAD_DIM)
    def _(h):
        cols = pl.ds(pl.multiple_of(h * HEAD_DIM, HEAD_DIM), HEAD_DIM)
        kept = inner_ref[:, cols] + dot(lead_ref[:, cols], enter_ref[cols, :])
        centred = kept - jnp.mean(kept, axis=-1, keepdims=True)
        variance = jnp.mean(centred * centred, axis=-1, keepdims=True)
        gate = gate_ref[:, cols].astype(F32)
        opened = gate / (1.0 + jnp.exp(-gate))
        scaled = centred * lax.rsqrt(variance + group_eps)
        hidden_ref[:, cols] = (scaled * gain_ref[:, cols] * opened).astype(BF16)

    step = 512

    @pl.loop(0, out_ref.shape[1] // step)
    def _(n):
        cols = pl.ds(pl.multiple_of(n * step, step), step)
        out_ref[:, cols] = dot(hidden_ref[...], weight_ref[:, cols]).astype(BF16)


def norm_kernel(sum_ref, residual_ref, gain_ref, routes_ref, shares_ref, updated_ref, out_ref):
    updated = residual_ref[...].astype(F32)
    for i in range(sum_ref.shape[0]):
        updated = updated + sum_ref[i].astype(F32)
    updated_ref[...] = updated
    factor = lax.rsqrt(jnp.mean(updated * updated, axis=-1, keepdims=True) + square_eps)
    width = updated.shape[1]
    scaled = (updated * factor * gain_ref[...]).astype(BF16)
    rows = updated.shape[0]
    lane = iota((rows, WIDE), 1)
    expert = lane % (WIDE // 2)
    table = jnp.zeros((rows, WIDE), F32)
    for k in range(TOPK):
        table = table + jnp.where(routes_ref[:, k : k + 1] == expert, shares_ref[:, k : k + 1], 0.0)
    first = table.astype(BF16).astype(F32)
    noted = jnp.where(lane < WIDE // 2, first, table - first).astype(BF16)
    out_ref[:, 0:width] = scaled
    out_ref[:, width : width + WIDE] = noted


def lane_of(dest, place, half):
    return (dest // 2) * 8 + place * 2 + dest % 2 + half * (WIDE // 2)


def gather_kernel(chunk, place_ref, *refs):
    blocks, out_ref = refs[:-1], refs[-1]
    block = blocks[0].shape[0]
    width = out_ref.shape[1]
    dests = out_ref.shape[0] // TILE
    place = place_ref[0]
    choose = (iota((dests, WIDE), 1) == lane_of(iota((dests, WIDE), 0), place, 0)).astype(BF16)
    earlier = (iota((block, block), 0) < iota((block, block), 1)).astype(BF16)
    line = iota((dests, TILE, block), 1)
    picks = []
    for i, ref in enumerate(blocks):
        named = (dot(choose, ref[:, width : width + WIDE], 1, 1) > 0.0).astype(F32)
        slot = dot(named.astype(BF16), earlier).astype(jnp.int32) + (CAP * (chunk + i) - TILE * chunk)
        slot = jnp.where(named > 0.0, slot, -1)
        pick = (slot[:, None, :] == line).astype(F32).reshape(dests * TILE, block)
        picks.append(pick.astype(BF16))
    pick = jnp.concatenate(picks, axis=1)
    step = 256

    @pl.loop(0, width // step)
    def _(n):
        cols = pl.ds(pl.multiple_of(n * step, step), step)
        rows = jnp.concatenate([ref[:, cols] for ref in blocks], axis=0)
        out_ref[:, cols] = dot(pick, rows).astype(BF16)


def merge_kernel(first_block, place_ref, *refs):
    count = 2
    tables, outs = refs[:count], refs[-count:]
    backs = refs[count:-count]
    block, dests = tables[0].shape[0], backs[0].shape[0] // TILE
    place = place_ref[0]
    earlier = (iota((block, block), 1) < iota((block, block), 0)).astype(BF16)
    spread = (iota((dests, dests * TILE), 1) // TILE == iota((dests, dests * TILE), 0)).astype(BF16)
    place_in = iota((block, dests * TILE), 1) % TILE
    mixes = []
    for i, table_ref in enumerate(tables):
        table = table_ref[...]
        high, low = [
            dot(table, (iota((WIDE, dests), 0) == lane_of(iota((WIDE, dests), 1), place, half)).astype(BF16))
            for half in (0, 1)
        ]
        slot = dot(earlier, (high > 0.0).astype(F32).astype(BF16)) + CAP * (first_block + i)
        slot_wide = dot(slot.astype(BF16), spread).astype(jnp.int32)
        parts = [dot(part.astype(BF16), spread) for part in (high, low)]
        chunk_base = first_block // 2
        mixes.append(
            [
                jnp.concatenate(
                    [
                        jnp.where(slot_wide == place_in + (chunk_base + c) * TILE, part, 0.0).astype(BF16)
                        for c in range(len(backs))
                    ],
                    axis=1,
                )
                for part in parts
            ]
        )
    high = jnp.concatenate([pair[0] for pair in mixes], axis=0)
    low = jnp.concatenate([pair[1] for pair in mixes], axis=0)
    step = 256

    @pl.loop(0, outs[0].shape[1] // step)
    def _(n):
        cols = pl.ds(pl.multiple_of(n * step, step), step)
        piece = jnp.concatenate([ref[:, cols] for ref in backs], axis=0)
        total = (dot(high, piece) + dot(low, piece)).astype(BF16)
        for i, out_ref in enumerate(outs):
            out_ref[:, cols] = total[i * block : (i + 1) * block]


def expert_kernel(parts, *refs):
    ins, (gate_ref, up_ref, down_ref) = refs[:parts], refs[parts : parts + 3]
    outs = refs[parts + 3 : -6]
    all_ref, act_ref, gate_in, up_in, down_in, sems = refs[-6:]
    rows = ins[0].shape[0]
    fetches = [
        [
            pltpu.make_async_copy(
                source.at[0, pl.ds(j * (target.shape[0] // PIECES), target.shape[0] // PIECES)],
                target.at[pl.ds(j * (target.shape[0] // PIECES), target.shape[0] // PIECES)],
                sems.at[i, j],
            )
            for j in range(PIECES)
        ]
        for i, (source, target) in enumerate(((gate_ref, gate_in), (up_ref, up_in), (down_ref, down_in)))
    ]
    for group in fetches:
        for fetch in group:
            fetch.start()
    for i, ref in enumerate(ins):
        all_ref[i * rows : (i + 1) * rows, :] = ref[...]
    for fetch in fetches[0]:
        fetch.wait()
    for fetch in fetches[1]:
        fetch.wait()
    half = 256

    @pl.loop(0, gate_in.shape[1] // half)
    def _(n):
        cols = pl.ds(pl.multiple_of(n * half, half), half)
        gate = jnp.minimum(dot(all_ref[...], gate_in[:, cols]), clamp_limit)
        gate = gate / (1.0 + jnp.exp(-swish_alpha * gate))
        up = jnp.clip(dot(all_ref[...], up_in[:, cols]), -clamp_limit, clamp_limit)
        act_ref[:, cols] = ((up + 1.0) * gate).astype(BF16)

    for fetch in fetches[2]:
        fetch.wait()
    step = 512

    @pl.loop(0, down_in.shape[1] // step)
    def _(n):
        cols = pl.ds(pl.multiple_of(n * step, step), step)
        part = dot(act_ref[...], down_in[:, cols]).astype(BF16)
        for i, out_ref in enumerate(outs):
            out_ref[:, cols] = part[i * rows : (i + 1) * rows]


def experts(rows, weights):
    count, width = rows[0].shape
    total, hidden = count * len(rows), weights[0].shape[2]
    return call(
        functools.partial(expert_kernel, len(rows)),
        [shape((count, width))] * len(rows),
        *rows, *weights,
        flops=6 * total * width * hidden,
        far=range(len(rows), len(rows) + 3),
        room=56,
        scratch=[
            pltpu.VMEM((total, width), BF16),
            pltpu.VMEM((total, hidden), BF16),
            pltpu.VMEM((width, hidden), BF16),
            pltpu.VMEM((width, hidden), BF16),
            pltpu.VMEM((hidden, width), BF16),
            pltpu.SemaphoreType.DMA((3, PIECES)),
        ],
    )


def ring(size, shift):
    return [(i, (i + shift) % size) for i in range(size)]


def add(a, b):
    return (a.astype(F32) + b.astype(F32)).astype(BF16)


def body(
    query_rows,
    key_rows,
    value_rows,
    gate_rows,
    log_decay,
    head_gain,
    out_weight,
    residual,
    ffn_gain,
    gate_weight,
    up_weight,
    down_weight,
    routes,
    route_weights,
):
    tok_count, heads = log_decay.shape
    local = heads * HEAD_DIM
    rows_own, width = residual.shape
    sp_count = lax.axis_size(SP)
    tp_count = lax.axis_size("tp")
    sp_index = lax.axis_index(SP)

    inverse = rope_base ** (-np.arange(HALF, dtype=np.float64) / HALF)
    inside = np.arange(tok_count, dtype=np.float64)[:, None] * inverse[None]
    starts = (np.arange(sp_count, dtype=np.float64) * tok_count)[:, None] * np.tile(inverse, 2)[None]
    cos_own, sin_own = jnp.asarray(np.cos(inside), F32), jnp.asarray(np.sin(inside), F32)
    base_all = jnp.asarray(np.stack([np.cos(starts), np.sin(starts)], axis=1), F32)
    base = lax.dynamic_index_in_dim(base_all, sp_index, 0, keepdims=False)

    near_count = lax.axis_size(("x", "c"))
    far_count = lax.axis_size("z")
    share = local // near_count
    message = call(
        state_kernel,
        shape((near_count, share + TILE, HEAD_DIM)),
        key_rows, value_rows, log_decay, cos_own, sin_own, base,
        flops=2 * tok_count * local * HEAD_DIM,
    )
    spans = lax.all_to_all(message, ("x", "c"), 0, 0, tiled=True)
    inner, lead = call(
        inner_kernel,
        [shape((tok_count, local), F32), shape((tok_count, local))],
        query_rows, key_rows, value_rows, log_decay, cos_own, sin_own, base,
        flops=4 * tok_count * tok_count * local,
        scratch=[pltpu.VMEM((heads, tok_count), F32)],
    )
    before, reach, group = call(
        group_kernel,
        [shape((near_count, share, HEAD_DIM), F32), shape((near_count, TILE, HEAD_DIM), F32), shape((far_count, share + TILE, HEAD_DIM))],
        spans,
    )
    groups = lax.all_to_all(group, "z", 0, 0, tiled=True)
    entering = call(
        enter_kernel,
        shape((near_count, share, HEAD_DIM)),
        lax.axis_index("z").astype(jnp.int32).reshape(1), groups, before, reach,
        smem=(0,),
    )
    entering = lax.all_to_all(entering, ("x", "c"), 0, 0, tiled=True).reshape(local, HEAD_DIM)
    mixed = call(
        mix_kernel,
        shape((tok_count, width)),
        inner, lead, entering, gate_rows, head_gain.reshape(1, local), out_weight,
        flops=2 * tok_count * local * width,
        scratch=[pltpu.VMEM((tok_count, local), BF16)],
    )
    pieces = lax.all_to_all(mixed.reshape(tp_count, rows_own, width), "tp", 0, 0, tiled=True)
    own_routes = lax.dynamic_slice_in_dim(routes, lax.axis_index("tp") * rows_own, rows_own, 0)
    updated, extended = call(
        norm_kernel,
        [shape((rows_own, width), F32), shape((rows_own, width + WIDE))],
        pieces, residual, ffn_gain.reshape(1, width), own_routes, route_weights,
    )

    place = lax.axis_index("x").astype(jnp.int32).reshape(1)
    x_count = lax.axis_size("x")
    shifts = range(x_count)
    near = [extended]
    for d in shifts[1:]:
        near.append(lax.ppermute(extended, "x", ring(x_count, -d)))
    dests = sp_count // x_count
    chunks = x_count * CAP // TILE
    outgoing = []
    for c in range(chunks):
        outgoing.append(
            call(
                functools.partial(gather_kernel, c),
                shape((dests * TILE, width)),
                place, near[c], near[c + 1],
                flops=4 * dests * TILE * rows_own * width,
                smem=(0,),
            )
        )
    weights = gate_weight, up_weight, down_weight
    ahead, behind = ring(tp_count, 1), ring(tp_count, -1)
    returned = []
    for c, piece in enumerate(outgoing, 1):
        first, second = (ahead, behind) if c % 2 else (behind, ahead)
        own = lax.all_to_all(piece.reshape(dests, TILE, width), ("z", "c"), 0, 0, tiled=True)
        own = own.reshape(dests * TILE, width)
        one = lax.ppermute(own, "tp", first)
        two = lax.ppermute(own, "tp", second)
        far = lax.ppermute(one, "tp", first)
        out_own, out_one, out_two = experts([own, one, two], weights)
        (out_far,) = experts([far], weights)
        via = lax.ppermute(out_far, "tp", second)
        back_one = lax.ppermute(add(out_one, via), "tp", second)
        back_two = lax.ppermute(out_two, "tp", first)
        total = (out_own.astype(F32) + back_one.astype(F32) + back_two.astype(F32)).astype(BF16)
        back = lax.all_to_all(total.reshape(dests, TILE, width), ("z", "c"), 0, 0, tiled=True)
        returned.append(back.reshape(dests * TILE, width))
    tables = [rows[:, width:] for rows in near]
    merged = []
    for i in range(2):
        merged += call(
            functools.partial(merge_kernel, 2 * i),
            [shape((rows_own, width))] * 2,
            place, tables[2 * i], tables[2 * i + 1], returned[i], returned[i + 1],
            flops=8 * dests * TILE * rows_own * width,
            smem=(0,),
        )
    total = updated + merged[0].astype(F32)
    for d in shifts[1:]:
        total = total + lax.ppermute(merged[d], "x", ring(x_count, d)).astype(F32)
    return total.astype(BF16)


def solution(mesh):
    finer = Mesh(mesh.devices.reshape(8, 4, 2, mesh.shape["tp"]), SP_TP)
    return jax.shard_map(
        body,
        mesh=finer,
        in_specs=(
            P(SP, "tp"),
            P(SP, "tp"),
            P(SP, "tp"),
            P(SP, "tp"),
            P(SP, "tp"),
            P("tp"),
            P("tp", None),
            P(SP_TP, None),
            P(),
            P(SP, None, "tp"),
            P(SP, None, "tp"),
            P(SP, "tp", None),
            P(SP, None),
            P(SP_TP, None),
        ),
        out_specs=P(SP_TP, None),
        check_vma=False,
    )
```

```python
import functools
import math

import jax
import jax.numpy as jnp
import numpy as np
from jax import lax
from jax.experimental import pallas as pl
from jax.experimental.pallas import tpu as pltpu
from jax.sharding import Mesh
from jax.sharding import PartitionSpec as P


HEAD_DIM = 128
HALF = HEAD_DIM // 2
TOPK = 4
SP = ("z", "x", "c")
SP_TP = ("z", "x", "c", "tp")
CAP = 6
TILE = 8
WIDE = 128
SPARE = TILE - CAP
WHOLE = (0, 2, 3)

rope_base = 10000.0
group_eps = 1e-05
square_eps = 1e-06
clamp_limit = 7.0
swish_alpha = 1.702

F32 = jnp.float32
BF16 = jnp.bfloat16


def dims(lhs, rhs):
    return (((lhs,), (rhs,)), ((), ()))


def dot(a, b, lhs=1, rhs=0):
    return lax.dot_general(a, b, dims(lhs, rhs), preferred_element_type=F32)


def iota(shape, dim):
    return lax.broadcasted_iota(jnp.int32, shape, dim)


def call(kernel, out_shape, *args, flops=0, smem=(), far=(), scratch=(), room=24):
    moved = sum(math.prod(a.shape) * a.dtype.itemsize for a in args)
    specs = [
        pl.BlockSpec(memory_space=pltpu.SMEM if i in smem else pltpu.HBM if i in far else pltpu.VMEM)
        for i in range(len(args))
    ]
    multi = isinstance(out_shape, (list, tuple))
    outs = [pl.BlockSpec(memory_space=pltpu.VMEM)] * len(out_shape) if multi else pl.BlockSpec(memory_space=pltpu.VMEM)
    return pl.pallas_call(
        kernel,
        out_shape=out_shape,
        in_specs=specs,
        out_specs=outs,
        scratch_shapes=list(scratch),
        compiler_params=pltpu.CompilerParams(vmem_limit_bytes=room * 1024 * 1024),
        cost_estimate=pl.CostEstimate(flops=flops, bytes_accessed=moved, transcendentals=0),
    )(*args)


def shape(dims_, kind=BF16):
    return jax.ShapeDtypeStruct(dims_, kind)


def three_parts(value):
    first = value.astype(BF16)
    rest = value - first.astype(F32)
    second = rest.astype(BF16)
    return first, second, (rest - second.astype(F32)).astype(BF16)


def tables(index_ref, own_ref, base_ref):
    parts = []
    for table in (own_ref[...], base_ref[pl.ds(index_ref[0], 1), :]):
        for half in (table[:, :HALF], table[:, HALF:]):
            parts.append(jnp.concatenate([half, half], axis=1))
    cos_own, sin_own, cos_base, sin_base = parts
    cosine = cos_base * cos_own - sin_base * sin_own
    sine = sin_base * cos_own + cos_base * sin_own
    return cosine, jnp.where(iota(sine.shape, 1) < HALF, -sine, sine)


def turned(values, cosine, sine):
    return values * cosine + pltpu.roll(values, HALF, 1) * sine


def state_kernel(index_ref, k_ref, v_ref, decay_ref, own_ref, base_ref, out_ref):
    heads, rows = decay_ref.shape
    cosine, sine = tables(index_ref, own_ref, base_ref)
    lower = (iota((rows, rows), 0) >= iota((rows, rows), 1)).astype(BF16)
    cumulative = sum(dot(lower, part, 1, 1) for part in three_parts(decay_ref[...]))
    share = out_ref.shape[1] - TILE
    per_head = HEAD_DIM // share
    lane = iota((rows, heads), 1)

    @pl.loop(0, heads)
    def _(h):
        cols = pl.ds(pl.multiple_of(h * HEAD_DIM, HEAD_DIM), HEAD_DIM)
        keys = turned(k_ref[:, cols].astype(F32), cosine, sine) * HEAD_DIM ** (-0.5)
        column = jnp.sum(jnp.where(lane == h, cumulative, 0.0), axis=1, keepdims=True)
        total = column[rows - 1 : rows, :]
        tail = keys * jnp.exp(total - column)
        state = dot(tail.astype(BF16), v_ref[:, cols], 0, 0)
        for i in range(per_head):
            out_ref[h * per_head + i, 0:share, :] = state[i * share : (i + 1) * share].astype(BF16)
            out_ref[h * per_head + i, share : share + TILE, :] = note_of(total)


def note_of(total):
    line = iota((TILE, HEAD_DIM), 0)
    first, second, third = [p.astype(F32) for p in three_parts(total)]
    note = jnp.where(line == 0, first, jnp.where(line == 1, second, jnp.where(line == 2, third, 0.0)))
    return note.astype(BF16)


def total_of(note):
    return note[0:1] + note[1:2] + note[2:3]


def group_kernel(in_ref, before_ref, reach_ref, out_ref):
    share = in_ref.shape[1] - TILE
    state = jnp.zeros((share, HEAD_DIM), F32)
    reach = jnp.zeros((1, HEAD_DIM), F32)
    for j in range(in_ref.shape[0]):
        before_ref[j] = state
        reach_ref[j] = jnp.broadcast_to(reach, (TILE, HEAD_DIM))
        piece = in_ref[j].astype(F32)
        total = total_of(piece[share:])
        state = state * jnp.exp(total) + piece[:share]
        reach = reach + total
    for i in range(out_ref.shape[0]):
        out_ref[i, 0:share, :] = state.astype(BF16)
        out_ref[i, share:, :] = note_of(reach)


def enter_kernel(place_ref, in_ref, before_ref, reach_ref, out_ref):
    share = out_ref.shape[1]
    place = place_ref[0]
    state = jnp.zeros((share, HEAD_DIM), F32)
    for j in range(in_ref.shape[0]):
        piece = in_ref[j].astype(F32)
        later = state * jnp.exp(total_of(piece[share:])) + piece[:share]
        state = jnp.where(j < place, later, state)
    for j in range(out_ref.shape[0]):
        out_ref[j] = (state * jnp.exp(reach_ref[j, 0:1]) + before_ref[j]).astype(BF16)


def inner_kernel(index_ref, q_ref, k_ref, v_ref, decay_ref, own_ref, base_ref, out_ref, lead_ref, across_ref):
    heads, rows = decay_ref.shape
    cosine, sine = tables(index_ref, own_ref, base_ref)
    causal = iota((rows, rows), 0) >= iota((rows, rows), 1)
    lower = causal.astype(BF16)
    parts = three_parts(decay_ref[...])
    cumulative = sum(dot(lower, part, 1, 1) for part in parts)
    across = sum(dot(part, lower, 1, 1) for part in parts)
    across_ref[...] = across
    lane = iota((rows, heads), 1)

    @pl.loop(0, heads)
    def _(h):
        cols = pl.ds(pl.multiple_of(h * HEAD_DIM, HEAD_DIM), HEAD_DIM)
        keys = turned(k_ref[:, cols].astype(F32), cosine, sine) * HEAD_DIM ** (-0.5)
        queries = turned(q_ref[:, cols].astype(F32), cosine, sine)
        column = jnp.sum(jnp.where(lane == h, cumulative, 0.0), axis=1, keepdims=True)
        gap = column - across_ref[pl.ds(h, 1), :]
        weights = jnp.where(causal, jnp.exp(jnp.minimum(gap, 0.0)), 0.0)
        scores = dot(queries.astype(BF16), keys.astype(BF16), 1, 1) * weights
        out_ref[:, cols] = dot(scores.astype(BF16), v_ref[:, cols])
        lead_ref[:, cols] = (queries * jnp.exp(column)).astype(BF16)


def mix_kernel(inner_ref, lead_ref, enter_ref, gate_ref, gain_ref, weight_ref, out_ref, hidden_ref):
    @pl.loop(0, inner_ref.shape[1] // HEAD_DIM)
    def _(h):
        cols = pl.ds(pl.multiple_of(h * HEAD_DIM, HEAD_DIM), HEAD_DIM)
        kept = inner_ref[:, cols] + dot(lead_ref[:, cols], enter_ref[cols, :])
        centred = kept - jnp.mean(kept, axis=-1, keepdims=True)
        variance = jnp.mean(centred * centred, axis=-1, keepdims=True)
        gate = gate_ref[:, cols].astype(F32)
        opened = gate / (1.0 + jnp.exp(-gate))
        scaled = centred * lax.rsqrt(variance + group_eps)
        hidden_ref[:, cols] = (scaled * gain_ref[:, cols] * opened).astype(BF16)

    step = 512

    @pl.loop(0, out_ref.shape[1] // step)
    def _(n):
        cols = pl.ds(pl.multiple_of(n * step, step), step)
        out_ref[:, cols] = dot(hidden_ref[...], weight_ref[:, cols]).astype(BF16)


def norm_kernel(sum_ref, residual_ref, gain_ref, routes_ref, shares_ref, updated_ref, out_ref):
    updated = residual_ref[...].astype(F32)
    for i in range(sum_ref.shape[0]):
        updated = updated + sum_ref[i].astype(F32)
    updated_ref[...] = updated
    factor = lax.rsqrt(jnp.mean(updated * updated, axis=-1, keepdims=True) + square_eps)
    width = updated.shape[1]
    scaled = (updated * factor * gain_ref[...]).astype(BF16)
    rows = updated.shape[0]
    lane = iota((rows, WIDE), 1)
    expert = lane % (WIDE // 2)
    table = jnp.zeros((rows, WIDE), F32)
    for k in range(TOPK):
        table = table + jnp.where(routes_ref[:, k : k + 1] == expert, shares_ref[:, k : k + 1], 0.0)
    first = table.astype(BF16).astype(F32)
    noted = jnp.where(lane < WIDE // 2, first, table - first).astype(BF16)
    out_ref[:, 0:width] = scaled
    out_ref[:, width : width + WIDE] = noted


def lane_of(dest, place, half):
    return (dest // 2) * 8 + place * 2 + dest % 2 + half * (WIDE // 2)


def gather_kernel(chunk, place_ref, *refs):
    blocks, out_ref = refs[:-1], refs[-1]
    block = blocks[0].shape[0]
    width = out_ref.shape[1]
    dests = out_ref.shape[0] // TILE
    place = place_ref[0]
    choose = (iota((dests, WIDE), 1) == lane_of(iota((dests, WIDE), 0), place, 0)).astype(BF16)
    earlier = (iota((block, block), 0) < iota((block, block), 1)).astype(BF16)
    line = iota((dests, TILE, block), 1)
    picks = []
    for i, ref in enumerate(blocks):
        named = dot(choose, ref[:, width : width + WIDE], 1, 1) > 0.0
        slot = dot(named.astype(F32).astype(BF16), earlier).astype(jnp.int32)
        if i == 1:
            slot = slot + (CAP - SPARE * chunk)
            named = named & (slot >= CAP)
        slot = jnp.where(named, slot, -1)
        pick = (slot[:, None, :] == line).astype(F32).reshape(dests * TILE, block)
        picks.append(pick.astype(BF16))
    pick = jnp.concatenate(picks, axis=1)
    step = 256

    @pl.loop(0, width // step)
    def _(n):
        cols = pl.ds(pl.multiple_of(n * step, step), step)
        rows = jnp.concatenate([ref[:, cols] for ref in blocks], axis=0)
        out_ref[:, cols] = dot(pick, rows).astype(BF16)


def merge_kernel(uses, place_ref, *refs):
    count = len(uses)
    tables, outs = refs[:count], refs[-count:]
    backs = refs[count:-count]
    block, dests = tables[0].shape[0], backs[0].shape[0] // TILE
    place = place_ref[0]
    earlier = (iota((block, block), 1) < iota((block, block), 0)).astype(BF16)
    spread = (iota((dests, dests * TILE), 1) // TILE == iota((dests, dests * TILE), 0)).astype(BF16)
    place_in = iota((block, dests * TILE), 1) % TILE
    mixes = []
    for table_ref, own_uses in zip(tables, uses):
        table = table_ref[...]
        high, low = [
            dot(table, (iota((WIDE, dests), 0) == lane_of(iota((WIDE, dests), 1), place, half)).astype(BF16))
            for half in (0, 1)
        ]
        rank = dot(earlier, (high > 0.0).astype(F32).astype(BF16))
        rank = dot(rank.astype(BF16), spread).astype(jnp.int32)
        parts = [dot(part.astype(BF16), spread) for part in (high, low)]
        lines = []
        for _, spare in own_uses:
            if spare is None:
                lines.append((rank == place_in) & (place_in < CAP))
            else:
                lines.append((rank == place_in - (CAP - SPARE * spare)) & (place_in >= CAP))
        mixes.append(
            [
                jnp.concatenate([jnp.where(here, part, 0.0).astype(BF16) for here in lines], axis=1)
                for part in parts
            ]
        )
    step = 256

    @pl.loop(0, outs[0].shape[1] // step)
    def _(n):
        cols = pl.ds(pl.multiple_of(n * step, step), step)
        for (high, low), own_uses, out_ref in zip(mixes, uses, outs):
            piece = jnp.concatenate([backs[i][:, cols] for i, _ in own_uses], axis=0)
            out_ref[:, cols] = (dot(high, piece) + dot(low, piece)).astype(BF16)


def expert_kernel(parts, *refs):
    ins, (gate_ref, up_ref, down_ref) = refs[:parts], refs[parts : parts + 3]
    outs = refs[parts + 3 : -6]
    all_ref, act_ref, open_ref, up_in, down_in, sems = refs[-6:]
    rows = ins[0].shape[0]
    fetch_up = pltpu.make_async_copy(up_ref.at[0], up_in, sems.at[0])
    fetch_down = pltpu.make_async_copy(down_ref.at[0], down_in, sems.at[1])
    fetch_up.start()
    fetch_down.start()
    for i, ref in enumerate(ins):
        all_ref[i * rows : (i + 1) * rows, :] = ref[...]
    half = 256

    @pl.loop(0, up_in.shape[1] // half)
    def _(n):
        cols = pl.ds(pl.multiple_of(n * half, half), half)
        gate = jnp.minimum(dot(all_ref[...], gate_ref[0, :, cols]), clamp_limit)
        open_ref[:, cols] = gate / (1.0 + jnp.exp(-swish_alpha * gate))

    fetch_up.wait()

    @pl.loop(0, up_in.shape[1] // half)
    def _(n):
        cols = pl.ds(pl.multiple_of(n * half, half), half)
        up = jnp.clip(dot(all_ref[...], up_in[:, cols]), -clamp_limit, clamp_limit)
        act_ref[:, cols] = ((up + 1.0) * open_ref[:, cols]).astype(BF16)

    fetch_down.wait()
    step = 512

    @pl.loop(0, down_in.shape[1] // step)
    def _(n):
        cols = pl.ds(pl.multiple_of(n * step, step), step)
        part = dot(act_ref[...], down_in[:, cols]).astype(BF16)
        for i, out_ref in enumerate(outs):
            out_ref[:, cols] = part[i * rows : (i + 1) * rows]


def experts(rows, weights):
    count, width = rows[0].shape
    total, hidden = count * len(rows), weights[0].shape[2]
    return call(
        functools.partial(expert_kernel, len(rows)),
        [shape((count, width))] * len(rows),
        *rows, *weights,
        flops=6 * total * width * hidden,
        far=range(len(rows) + 1, len(rows) + 3),
        room=50,
        scratch=[
            pltpu.VMEM((total, width), BF16),
            pltpu.VMEM((total, hidden), BF16),
            pltpu.VMEM((total, hidden), F32),
            pltpu.VMEM((width, hidden), BF16),
            pltpu.VMEM((hidden, width), BF16),
            pltpu.SemaphoreType.DMA((2,)),
        ],
    )


def ring(size, shift):
    return [(i, (i + shift) % size) for i in range(size)]


def add(a, b):
    return (a.astype(F32) + b.astype(F32)).astype(BF16)


def body(
    query_rows,
    key_rows,
    value_rows,
    gate_rows,
    log_decay,
    head_gain,
    out_weight,
    residual,
    ffn_gain,
    gate_weight,
    up_weight,
    down_weight,
    routes,
    route_weights,
):
    tok_count, heads = log_decay.shape
    local = heads * HEAD_DIM
    rows_own, width = residual.shape
    sp_count = lax.axis_size(SP)
    tp_count = lax.axis_size("tp")
    sp_index = lax.axis_index(SP)

    inverse = rope_base ** (-np.arange(HALF, dtype=np.float64) / HALF)
    inside = np.arange(tok_count, dtype=np.float64)[:, None] * inverse[None]
    starts = (np.arange(sp_count, dtype=np.float64) * tok_count)[:, None] * inverse[None]
    own_table, base = [
        jnp.asarray(np.concatenate([np.cos(angle), np.sin(angle)], axis=1), F32)
        for angle in (inside, starts)
    ]
    index = sp_index.astype(jnp.int32).reshape(1)
    decays = log_decay.T

    near_count = lax.axis_size(("x", "c"))
    far_count = lax.axis_size("z")
    share = local // near_count
    message = call(
        state_kernel,
        shape((near_count, share + TILE, HEAD_DIM)),
        index, key_rows, value_rows, decays, own_table, base,
        flops=2 * tok_count * local * HEAD_DIM,
        smem=(0,),
        room=56,
    )
    spans = lax.all_to_all(message, ("x", "c"), 0, 0, tiled=True)
    inner, lead = call(
        inner_kernel,
        [shape((tok_count, local), F32), shape((tok_count, local))],
        index, query_rows, key_rows, value_rows, decays, own_table, base,
        smem=(0,),
        flops=4 * tok_count * tok_count * local,
        room=56,
        scratch=[pltpu.VMEM((heads, tok_count), F32)],
    )
    before, reach, group = call(
        group_kernel,
        [shape((near_count, share, HEAD_DIM), F32), shape((near_count, TILE, HEAD_DIM), F32), shape((far_count, share + TILE, HEAD_DIM))],
        spans,
    )
    groups = lax.all_to_all(group, "z", 0, 0, tiled=True)
    entering = call(
        enter_kernel,
        shape((near_count, share, HEAD_DIM)),
        lax.axis_index("z").astype(jnp.int32).reshape(1), groups, before, reach,
        smem=(0,),
    )
    entering = lax.all_to_all(entering, ("x", "c"), 0, 0, tiled=True).reshape(local, HEAD_DIM)
    mixed = call(
        mix_kernel,
        shape((tok_count, width)),
        inner, lead, entering, gate_rows, head_gain.reshape(1, local), out_weight,
        flops=2 * tok_count * local * width,
        scratch=[pltpu.VMEM((tok_count, local), BF16)],
    )
    pieces = lax.all_to_all(mixed.reshape(tp_count, rows_own, width), "tp", 0, 0, tiled=True)
    own_routes = lax.dynamic_slice_in_dim(routes, lax.axis_index("tp") * rows_own, rows_own, 0)
    updated, extended = call(
        norm_kernel,
        [shape((rows_own, width), F32), shape((rows_own, width + WIDE))],
        pieces, residual, ffn_gain.reshape(1, width), own_routes, route_weights,
    )

    place = lax.axis_index("x").astype(jnp.int32).reshape(1)
    x_count = lax.axis_size("x")
    shifts = range(x_count)
    near = [extended]
    for d in shifts[1:]:
        near.append(lax.ppermute(extended, "x", ring(x_count, -d)))
    dests = sp_count // x_count
    chunks = x_count * CAP // TILE
    outgoing = []
    for c in range(chunks):
        outgoing.append(
            call(
                functools.partial(gather_kernel, c),
                shape((dests * TILE, width)),
                place, near[WHOLE[c]], near[1],
                flops=4 * dests * TILE * rows_own * width,
                smem=(0,),
            )
        )
    weights = pltpu.with_memory_space_constraint(gate_weight, pltpu.VMEM), up_weight, down_weight
    ahead, behind = ring(tp_count, 1), ring(tp_count, -1)
    returned = []
    for c, piece in enumerate(outgoing, 1):
        first, second = (ahead, behind) if c % 2 else (behind, ahead)
        own = lax.all_to_all(piece.reshape(dests, TILE, width), ("z", "c"), 0, 0, tiled=True)
        own = own.reshape(dests * TILE, width)
        one = lax.ppermute(own, "tp", first)
        two = lax.ppermute(own, "tp", second)
        far = lax.ppermute(one, "tp", first)
        out_own, out_one, out_two = experts([own, one, two], weights)
        (out_far,) = experts([far], weights)
        via = lax.ppermute(out_far, "tp", second)
        back_one = lax.ppermute(add(out_one, via), "tp", second)
        back_two = lax.ppermute(out_two, "tp", first)
        total = (out_own.astype(F32) + back_one.astype(F32) + back_two.astype(F32)).astype(BF16)
        back = lax.all_to_all(total.reshape(dests, TILE, width), ("z", "c"), 0, 0, tiled=True)
        returned.append(back.reshape(dests * TILE, width))
    tables = [rows[:, width:] for rows in near]

    def merge(blocks, uses, backs):
        return call(
            functools.partial(merge_kernel, uses),
            [shape((rows_own, width))] * len(blocks),
            place, *[tables[d] for d in blocks], *backs,
            flops=8 * dests * TILE * rows_own * width,
            smem=(0,),
        )

    merged = {}
    merged[0], merged[2] = merge((0, 2), (((0, None),), ((1, None),)), returned[:2])
    merged[1], merged[3] = merge((1, 3), (((0, 0), (1, 1), (2, 2)), ((2, None),)), returned)
    total = updated + merged[0].astype(F32)
    for d in (2, 1, 3):
        total = total + lax.ppermute(merged[d], "x", ring(x_count, d)).astype(F32)
    return total.astype(BF16)


def solution(mesh):
    finer = Mesh(mesh.devices.reshape(8, 4, 2, mesh.shape["tp"]), SP_TP)
    return jax.shard_map(
        body,
        mesh=finer,
        in_specs=(
            P(SP, "tp"),
            P(SP, "tp"),
            P(SP, "tp"),
            P(SP, "tp"),
            P(SP, "tp"),
            P("tp"),
            P("tp", None),
            P(SP_TP, None),
            P(),
            P(SP, None, "tp"),
            P(SP, None, "tp"),
            P(SP, "tp", None),
            P(SP, None),
            P(SP_TP, None),
        ),
        out_specs=P(SP_TP, None),
        check_vma=False,
    )
```

```python
import functools
import math

import jax
import jax.numpy as jnp
import numpy as np
from jax import lax
from jax.experimental import pallas as pl
from jax.experimental.pallas import tpu as pltpu
from jax.sharding import Mesh
from jax.sharding import PartitionSpec as P


HEAD_DIM = 128
HALF = HEAD_DIM // 2
TOPK = 4
SP = ("z", "x", "c")
SP_TP = ("z", "x", "c", "tp")
CAP = 6
TILE = 8
WIDE = 128
SPARE = TILE - CAP
WHOLE = (0, 2, 3)

rope_base = 10000.0
group_eps = 1e-05
square_eps = 1e-06
clamp_limit = 7.0
swish_alpha = 1.702

F32 = jnp.float32
BF16 = jnp.bfloat16


def dims(lhs, rhs):
    return (((lhs,), (rhs,)), ((), ()))


def dot(a, b, lhs=1, rhs=0):
    return lax.dot_general(a, b, dims(lhs, rhs), preferred_element_type=F32)


def iota(shape, dim):
    return lax.broadcasted_iota(jnp.int32, shape, dim)


def call(kernel, out_shape, *args, flops=0, smem=(), far=(), scratch=(), room=24):
    moved = sum(math.prod(a.shape) * a.dtype.itemsize for a in args)
    specs = [
        pl.BlockSpec(memory_space=pltpu.SMEM if i in smem else pltpu.HBM if i in far else pltpu.VMEM)
        for i in range(len(args))
    ]
    multi = isinstance(out_shape, (list, tuple))
    outs = [pl.BlockSpec(memory_space=pltpu.VMEM)] * len(out_shape) if multi else pl.BlockSpec(memory_space=pltpu.VMEM)
    return pl.pallas_call(
        kernel,
        out_shape=out_shape,
        in_specs=specs,
        out_specs=outs,
        scratch_shapes=list(scratch),
        compiler_params=pltpu.CompilerParams(vmem_limit_bytes=room * 1024 * 1024),
        cost_estimate=pl.CostEstimate(flops=flops, bytes_accessed=moved, transcendentals=0),
    )(*args)


def shape(dims_, kind=BF16):
    return jax.ShapeDtypeStruct(dims_, kind)


def three_parts(value):
    first = value.astype(BF16)
    rest = value - first.astype(F32)
    second = rest.astype(BF16)
    return first, second, (rest - second.astype(F32)).astype(BF16)


def tables(index_ref, own_ref, base_ref):
    parts = []
    for table in (own_ref[...], base_ref[pl.ds(index_ref[0], 1), :]):
        for half in (table[:, :HALF], table[:, HALF:]):
            parts.append(jnp.concatenate([half, half], axis=1))
    cos_own, sin_own, cos_base, sin_base = parts
    cosine = cos_base * cos_own - sin_base * sin_own
    sine = sin_base * cos_own + cos_base * sin_own
    return cosine, jnp.where(iota(sine.shape, 1) < HALF, -sine, sine)


def turned(values, cosine, sine):
    return values * cosine + pltpu.roll(values, HALF, 1) * sine


def state_kernel(index_ref, k_ref, v_ref, decay_ref, own_ref, base_ref, out_ref):
    heads, rows = decay_ref.shape
    cosine, sine = tables(index_ref, own_ref, base_ref)
    lower = (iota((rows, rows), 0) >= iota((rows, rows), 1)).astype(BF16)
    cumulative = sum(dot(lower, part, 1, 1) for part in three_parts(decay_ref[...]))
    share = out_ref.shape[1] - TILE
    per_head = HEAD_DIM // share
    for h in range(heads):
        cols = slice(h * HEAD_DIM, (h + 1) * HEAD_DIM)
        keys = turned(k_ref[:, cols].astype(F32), cosine, sine) * HEAD_DIM ** (-0.5)
        column = cumulative[:, h : h + 1]
        total = column[rows - 1 : rows, :]
        tail = keys * jnp.exp(total - column)
        state = dot(tail.astype(BF16), v_ref[:, cols], 0, 0)
        for i in range(per_head):
            out_ref[h * per_head + i, 0:share, :] = state[i * share : (i + 1) * share].astype(BF16)
            out_ref[h * per_head + i, share : share + TILE, :] = note_of(total)


def note_of(total):
    line = iota((TILE, HEAD_DIM), 0)
    first, second, third = [p.astype(F32) for p in three_parts(total)]
    note = jnp.where(line == 0, first, jnp.where(line == 1, second, jnp.where(line == 2, third, 0.0)))
    return note.astype(BF16)


def total_of(note):
    return note[0:1] + note[1:2] + note[2:3]


def group_kernel(in_ref, before_ref, reach_ref, out_ref):
    share = in_ref.shape[1] - TILE
    state = jnp.zeros((share, HEAD_DIM), F32)
    reach = jnp.zeros((1, HEAD_DIM), F32)
    for j in range(in_ref.shape[0]):
        before_ref[j] = state
        reach_ref[j] = jnp.broadcast_to(reach, (TILE, HEAD_DIM))
        piece = in_ref[j].astype(F32)
        total = total_of(piece[share:])
        state = state * jnp.exp(total) + piece[:share]
        reach = reach + total
    for i in range(out_ref.shape[0]):
        out_ref[i, 0:share, :] = state.astype(BF16)
        out_ref[i, share:, :] = note_of(reach)


def enter_kernel(place_ref, in_ref, before_ref, reach_ref, out_ref):
    share = out_ref.shape[1]
    place = place_ref[0]
    state = jnp.zeros((share, HEAD_DIM), F32)
    for j in range(in_ref.shape[0]):
        piece = in_ref[j].astype(F32)
        later = state * jnp.exp(total_of(piece[share:])) + piece[:share]
        state = jnp.where(j < place, later, state)
    for j in range(out_ref.shape[0]):
        out_ref[j] = (state * jnp.exp(reach_ref[j, 0:1]) + before_ref[j]).astype(BF16)


def inner_kernel(index_ref, q_ref, k_ref, v_ref, decay_ref, own_ref, base_ref, out_ref, lead_ref, across_ref):
    heads, rows = decay_ref.shape
    cosine, sine = tables(index_ref, own_ref, base_ref)
    causal = iota((rows, rows), 0) >= iota((rows, rows), 1)
    lower = causal.astype(BF16)
    parts = three_parts(decay_ref[...])
    cumulative = sum(dot(lower, part, 1, 1) for part in parts)
    across = sum(dot(part, lower, 1, 1) for part in parts)
    across_ref[...] = across
    lane = iota((rows, heads), 1)

    @pl.loop(0, heads)
    def _(h):
        cols = pl.ds(pl.multiple_of(h * HEAD_DIM, HEAD_DIM), HEAD_DIM)
        keys = turned(k_ref[:, cols].astype(F32), cosine, sine) * HEAD_DIM ** (-0.5)
        queries = turned(q_ref[:, cols].astype(F32), cosine, sine)
        column = jnp.sum(jnp.where(lane == h, cumulative, 0.0), axis=1, keepdims=True)
        gap = column - across_ref[pl.ds(h, 1), :]
        weights = jnp.where(causal, jnp.exp(jnp.minimum(gap, 0.0)), 0.0)
        scores = dot(queries.astype(BF16), keys.astype(BF16), 1, 1) * weights
        out_ref[:, cols] = dot(scores.astype(BF16), v_ref[:, cols])
        lead_ref[:, cols] = (queries * jnp.exp(column)).astype(BF16)


def mix_kernel(inner_ref, lead_ref, enter_ref, gate_ref, gain_ref, weight_ref, out_ref, hidden_ref):
    for h in range(inner_ref.shape[1] // HEAD_DIM):
        cols = slice(h * HEAD_DIM, (h + 1) * HEAD_DIM)
        kept = inner_ref[:, cols] + dot(lead_ref[:, cols], enter_ref[cols, :])
        centred = kept - jnp.mean(kept, axis=-1, keepdims=True)
        variance = jnp.mean(centred * centred, axis=-1, keepdims=True)
        gate = gate_ref[:, cols].astype(F32)
        opened = gate / (1.0 + jnp.exp(-gate))
        scaled = centred * lax.rsqrt(variance + group_eps)
        hidden_ref[:, cols] = (scaled * gain_ref[:, cols] * opened).astype(BF16)
    step = 512

    @pl.loop(0, out_ref.shape[1] // step)
    def _(n):
        cols = pl.ds(pl.multiple_of(n * step, step), step)
        out_ref[:, cols] = dot(hidden_ref[...], weight_ref[:, cols]).astype(BF16)


def norm_kernel(sum_ref, residual_ref, gain_ref, routes_ref, shares_ref, updated_ref, out_ref):
    updated = residual_ref[...].astype(F32)
    for i in range(sum_ref.shape[0]):
        updated = updated + sum_ref[i].astype(F32)
    updated_ref[...] = updated
    factor = lax.rsqrt(jnp.mean(updated * updated, axis=-1, keepdims=True) + square_eps)
    width = updated.shape[1]
    scaled = (updated * factor * gain_ref[...]).astype(BF16)
    rows = updated.shape[0]
    lane = iota((rows, WIDE), 1)
    expert = lane % (WIDE // 2)
    table = jnp.zeros((rows, WIDE), F32)
    for k in range(TOPK):
        table = table + jnp.where(routes_ref[:, k : k + 1] == expert, shares_ref[:, k : k + 1], 0.0)
    first = table.astype(BF16).astype(F32)
    noted = jnp.where(lane < WIDE // 2, first, table - first).astype(BF16)
    out_ref[:, 0:width] = scaled
    out_ref[:, width : width + WIDE] = noted


def lane_of(dest, place, half):
    return (dest // 2) * 8 + place * 2 + dest % 2 + half * (WIDE // 2)


def gather_kernel(chunk, place_ref, *refs):
    blocks, out_ref = refs[:-1], refs[-1]
    block = blocks[0].shape[0]
    width = out_ref.shape[1]
    dests = out_ref.shape[0] // TILE
    place = place_ref[0]
    choose = (iota((dests, WIDE), 1) == lane_of(iota((dests, WIDE), 0), place, 0)).astype(BF16)
    earlier = (iota((block, block), 0) < iota((block, block), 1)).astype(BF16)
    line = iota((dests, TILE, block), 1)
    picks = []
    for i, ref in enumerate(blocks):
        named = dot(choose, ref[:, width : width + WIDE], 1, 1) > 0.0
        slot = dot(named.astype(F32).astype(BF16), earlier).astype(jnp.int32)
        if i == 1:
            slot = slot + (CAP - SPARE * chunk)
            named = named & (slot >= CAP)
        slot = jnp.where(named, slot, -1)
        pick = (slot[:, None, :] == line).astype(F32).reshape(dests * TILE, block)
        picks.append(pick.astype(BF16))
    pick = jnp.concatenate(picks, axis=1)
    step = 512

    @pl.loop(0, width // step)
    def _(n):
        cols = pl.ds(pl.multiple_of(n * step, step), step)
        rows = jnp.concatenate([ref[:, cols] for ref in blocks], axis=0)
        out_ref[:, cols] = dot(pick, rows).astype(BF16)


def merge_kernel(uses, place_ref, *refs):
    count = len(uses)
    tables, outs = refs[:count], refs[-count:]
    backs = refs[count:-count]
    block, dests = tables[0].shape[0], backs[0].shape[0] // TILE
    place = place_ref[0]
    earlier = (iota((block, block), 1) < iota((block, block), 0)).astype(BF16)
    spread = (iota((dests, dests * TILE), 1) // TILE == iota((dests, dests * TILE), 0)).astype(BF16)
    place_in = iota((block, dests * TILE), 1) % TILE
    mixes = []
    for table_ref, own_uses in zip(tables, uses):
        table = table_ref[...]
        high, low = [
            dot(table, (iota((WIDE, dests), 0) == lane_of(iota((WIDE, dests), 1), place, half)).astype(BF16))
            for half in (0, 1)
        ]
        rank = dot(earlier, (high > 0.0).astype(F32).astype(BF16))
        rank = dot(rank.astype(BF16), spread).astype(jnp.int32)
        parts = [dot(part.astype(BF16), spread) for part in (high, low)]
        lines = []
        for _, spare in own_uses:
            if spare is None:
                lines.append((rank == place_in) & (place_in < CAP))
            else:
                lines.append((rank == place_in - (CAP - SPARE * spare)) & (place_in >= CAP))
        mixes.append(
            [
                jnp.concatenate([jnp.where(here, part, 0.0).astype(BF16) for here in lines], axis=1)
                for part in parts
            ]
        )
    step = 512

    @pl.loop(0, outs[0].shape[1] // step)
    def _(n):
        cols = pl.ds(pl.multiple_of(n * step, step), step)
        for (high, low), own_uses, out_ref in zip(mixes, uses, outs):
            piece = jnp.concatenate([backs[i][:, cols] for i, _ in own_uses], axis=0)
            out_ref[:, cols] = (dot(high, piece) + dot(low, piece)).astype(BF16)


def expert_kernel(parts, *refs):
    ins, (gate_ref, up_ref, down_ref) = refs[:parts], refs[parts : parts + 3]
    outs = refs[parts + 3 : -6]
    all_ref, act_ref, open_ref, up_in, down_in, sems = refs[-6:]
    rows = ins[0].shape[0]
    fetch_up = pltpu.make_async_copy(up_ref.at[0], up_in, sems.at[0])
    fetch_down = pltpu.make_async_copy(down_ref.at[0], down_in, sems.at[1])
    fetch_up.start()
    fetch_down.start()
    for i, ref in enumerate(ins):
        all_ref[i * rows : (i + 1) * rows, :] = ref[...]
    half = 256

    @pl.loop(0, up_in.shape[1] // half)
    def _(n):
        cols = pl.ds(pl.multiple_of(n * half, half), half)
        gate = jnp.minimum(dot(all_ref[...], gate_ref[0, :, cols]), clamp_limit)
        open_ref[:, cols] = gate / (1.0 + jnp.exp(-swish_alpha * gate))

    fetch_up.wait()

    @pl.loop(0, up_in.shape[1] // half)
    def _(n):
        cols = pl.ds(pl.multiple_of(n * half, half), half)
        up = jnp.clip(dot(all_ref[...], up_in[:, cols]), -clamp_limit, clamp_limit)
        act_ref[:, cols] = ((up + 1.0) * open_ref[:, cols]).astype(BF16)

    fetch_down.wait()
    step = 512

    @pl.loop(0, down_in.shape[1] // step)
    def _(n):
        cols = pl.ds(pl.multiple_of(n * step, step), step)
        part = dot(act_ref[...], down_in[:, cols]).astype(BF16)
        for i, out_ref in enumerate(outs):
            out_ref[:, cols] = part[i * rows : (i + 1) * rows]


def experts(rows, weights):
    count, width = rows[0].shape
    total, hidden = count * len(rows), weights[0].shape[2]
    return call(
        functools.partial(expert_kernel, len(rows)),
        [shape((count, width))] * len(rows),
        *rows, *weights,
        flops=6 * total * width * hidden,
        far=range(len(rows) + 1, len(rows) + 3),
        room=50,
        scratch=[
            pltpu.VMEM((total, width), BF16),
            pltpu.VMEM((total, hidden), BF16),
            pltpu.VMEM((total, hidden), F32),
            pltpu.VMEM((width, hidden), BF16),
            pltpu.VMEM((hidden, width), BF16),
            pltpu.SemaphoreType.DMA((2,)),
        ],
    )


def ring(size, shift):
    return [(i, (i + shift) % size) for i in range(size)]


def add(a, b):
    return (a.astype(F32) + b.astype(F32)).astype(BF16)


def body(
    query_rows,
    key_rows,
    value_rows,
    gate_rows,
    log_decay,
    head_gain,
    out_weight,
    residual,
    ffn_gain,
    gate_weight,
    up_weight,
    down_weight,
    routes,
    route_weights,
):
    tok_count, heads = log_decay.shape
    local = heads * HEAD_DIM
    rows_own, width = residual.shape
    sp_count = lax.axis_size(SP)
    tp_count = lax.axis_size("tp")
    sp_index = lax.axis_index(SP)

    inverse = rope_base ** (-np.arange(HALF, dtype=np.float64) / HALF)
    inside = np.arange(tok_count, dtype=np.float64)[:, None] * inverse[None]
    starts = (np.arange(sp_count, dtype=np.float64) * tok_count)[:, None] * inverse[None]
    own_table, base = [
        jnp.asarray(np.concatenate([np.cos(angle), np.sin(angle)], axis=1), F32)
        for angle in (inside, starts)
    ]
    index = sp_index.astype(jnp.int32).reshape(1)
    decays = log_decay.T

    near_count = lax.axis_size(("x", "c"))
    far_count = lax.axis_size("z")
    share = local // near_count
    message = call(
        state_kernel,
        shape((near_count, share + TILE, HEAD_DIM)),
        index, key_rows, value_rows, decays, own_table, base,
        flops=2 * tok_count * local * HEAD_DIM,
        smem=(0,),
        room=56,
    )
    spans = lax.all_to_all(message, ("x", "c"), 0, 0, tiled=True)
    inner, lead = call(
        inner_kernel,
        [shape((tok_count, local), F32), shape((tok_count, local))],
        index, query_rows, key_rows, value_rows, decays, own_table, base,
        smem=(0,),
        flops=4 * tok_count * tok_count * local,
        room=56,
        scratch=[pltpu.VMEM((heads, tok_count), F32)],
    )
    before, reach, group = call(
        group_kernel,
        [shape((near_count, share, HEAD_DIM), F32), shape((near_count, TILE, HEAD_DIM), F32), shape((far_count, share + TILE, HEAD_DIM))],
        spans,
    )
    groups = lax.all_to_all(group, "z", 0, 0, tiled=True)
    entering = call(
        enter_kernel,
        shape((near_count, share, HEAD_DIM)),
        lax.axis_index("z").astype(jnp.int32).reshape(1), groups, before, reach,
        smem=(0,),
    )
    entering = lax.all_to_all(entering, ("x", "c"), 0, 0, tiled=True).reshape(local, HEAD_DIM)
    mixed = call(
        mix_kernel,
        shape((tok_count, width)),
        inner, lead, entering, gate_rows, head_gain.reshape(1, local), out_weight,
        flops=2 * tok_count * local * width,
        scratch=[pltpu.VMEM((tok_count, local), BF16)],
    )
    pieces = lax.all_to_all(mixed.reshape(tp_count, rows_own, width), "tp", 0, 0, tiled=True)
    own_routes = lax.dynamic_slice_in_dim(routes, lax.axis_index("tp") * rows_own, rows_own, 0)
    updated, extended = call(
        norm_kernel,
        [shape((rows_own, width), F32), shape((rows_own, width + WIDE))],
        pieces, residual, ffn_gain.reshape(1, width), own_routes, route_weights,
    )

    place = lax.axis_index("x").astype(jnp.int32).reshape(1)
    x_count = lax.axis_size("x")
    shifts = range(x_count)
    near = [extended]
    for d in shifts[1:]:
        near.append(lax.ppermute(extended, "x", ring(x_count, -d)))
    dests = sp_count // x_count
    chunks = x_count * CAP // TILE
    outgoing = []
    for c in range(chunks):
        outgoing.append(
            call(
                functools.partial(gather_kernel, c),
                shape((dests * TILE, width)),
                place, near[WHOLE[c]], near[1],
                flops=4 * dests * TILE * rows_own * width,
                smem=(0,),
            )
        )
    weights = pltpu.with_memory_space_constraint(gate_weight, pltpu.VMEM), up_weight, down_weight
    ahead, behind = ring(tp_count, 1), ring(tp_count, -1)
    returned = []
    for c, piece in enumerate(outgoing, 1):
        first, second = (ahead, behind) if c % 2 else (behind, ahead)
        own = lax.all_to_all(piece.reshape(dests, TILE, width), ("z", "c"), 0, 0, tiled=True)
        own = own.reshape(dests * TILE, width)
        one = lax.ppermute(own, "tp", first)
        two = lax.ppermute(own, "tp", second)
        far = lax.ppermute(one, "tp", first)
        out_own, out_one, out_two = experts([own, one, two], weights)
        (out_far,) = experts([far], weights)
        via = lax.ppermute(out_far, "tp", second)
        back_one = lax.ppermute(add(out_one, via), "tp", second)
        back_two = lax.ppermute(out_two, "tp", first)
        total = (out_own.astype(F32) + back_one.astype(F32) + back_two.astype(F32)).astype(BF16)
        back = lax.all_to_all(total.reshape(dests, TILE, width), ("z", "c"), 0, 0, tiled=True)
        returned.append(back.reshape(dests * TILE, width))
    tables = [rows[:, width:] for rows in near]

    def merge(blocks, uses, backs):
        return call(
            functools.partial(merge_kernel, uses),
            [shape((rows_own, width))] * len(blocks),
            place, *[tables[d] for d in blocks], *backs,
            flops=8 * dests * TILE * rows_own * width,
            smem=(0,),
        )

    merged = {}
    merged[0], merged[2] = merge((0, 2), (((0, None),), ((1, None),)), returned[:2])
    merged[1], merged[3] = merge((1, 3), (((0, 0), (1, 1), (2, 2)), ((2, None),)), returned)
    total = updated + merged[0].astype(F32)
    for d in (2, 1, 3):
        total = total + lax.ppermute(merged[d], "x", ring(x_count, d)).astype(F32)
    return total.astype(BF16)


def solution(mesh):
    finer = Mesh(mesh.devices.reshape(8, 4, 2, mesh.shape["tp"]), SP_TP)
    return jax.shard_map(
        body,
        mesh=finer,
        in_specs=(
            P(SP, "tp"),
            P(SP, "tp"),
            P(SP, "tp"),
            P(SP, "tp"),
            P(SP, "tp"),
            P("tp"),
            P("tp", None),
            P(SP_TP, None),
            P(),
            P(SP, None, "tp"),
            P(SP, None, "tp"),
            P(SP, "tp", None),
            P(SP, None),
            P(SP_TP, None),
        ),
        out_specs=P(SP_TP, None),
        check_vma=False,
    )
```
